32 devices in a mesh: sp: 8 (over z, y), tp: 4 (over x, core).
Axes of the slice: x: 2, y: 2, z: 4, core: 2. Of those that a mesh axis runs over, the one named last changes fastest.
Arguments:
- tokens_in: bfloat16 [2048, 2048], P('sp'), may hold values from -6 to 6
- norm_gain: float32 [2048], replicated, may hold values from 0.1 to 1.9
- rec_query_weight: bfloat16 [2048, 1024], P('sp', 'tp'), may hold values from -0.125 to 0.125
- rec_forget_weight: bfloat16 [2048, 1024], P('sp', 'tp'), may hold values from -0.125 to 0.125
- rec_input_weight: bfloat16 [2048, 1024], P('sp', 'tp'), may hold values from -0.125 to 0.125
- att_query_weight: bfloat16 [2048, 1024], P('sp', 'tp'), may hold values from -0.18991481 to 0.18991481
- att_key_weight: bfloat16 [2048, 1024], P('sp', 'tp'), may hold values from -0.18991481 to 0.18991481
- att_value_weight: bfloat16 [2048, 1024], P('sp', 'tp'), may hold values from -0.125 to 0.125
- recurrence_output_weight: bfloat16 [1024, 2048], P('tp'), may hold values from -0.125 to 0.125
- out_att_weight: bfloat16 [1024, 2048], P('tp'), may hold values from -0.125 to 0.125
- floor_gap: float32 [1024], P('tp'), may hold values from 0 to 0.1
- decay_shift: float32 [8, 2048], P('tp', 'sp'), may hold values from -1.5 to 0
- rec_gain: float32 [128], replicated, may hold values from 0.1 to 1.9
- att_gain: float32 [128], replicated, may hold values from 0.1 to 1.9
- lambda_head: float32 [8], P('tp'), may hold values from 0.3 to 0.8
Outputs:
- mixed: bfloat16 [2048, 2048], P('sp')
The draws below stay inside these ranges and needn't reach their ends.
All inputs are finite; a program needn't handle non-finite values.
Results may differ from the reference program's by a relative error of at most 0.015.
Values may be sent and summed in bfloat16 or wider, within the bound.
A program may use at most 128 MiB of HBM per device.

```python
import math
import jax
import jax.numpy as jnp
from jax import lax

D = 2048
REC_HEADS = 8
REC_KEY = 128
REC_VAL = 128
ATT_HEADS = 8
PAIR = 64
ATT_VAL = 128
BLOCK = 64
TOK_DEV = 256
SEQS = 3
SEQ_LEN = 512
TOKENS = 2048
REC_WIDTH = 1024
ATT_WIDTH = 1024
N_TP = 4


def score_matrix(key, salt):
    normal = jax.random.normal(jax.random.fold_in(key, salt), (D, ATT_HEADS * 2 * PAIR), jnp.float32)
    return jnp.clip(normal, -4.0, 4.0) * (1.32 / math.sqrt(D))


def draw_tokens_in(key, part):
    noise_key = jax.random.fold_in(key, 11)
    return jnp.clip(jax.random.normal(noise_key, (TOKENS, D), jnp.float32), -6.0, 6.0).astype(jnp.bfloat16)


def draw_att_query_weight(key, part):
    matrix = score_matrix(key, 21)
    return matrix.astype(jnp.bfloat16)


def draw_att_key_weight(key, part):
    matrix = score_matrix(key, 22)
    return matrix.astype(jnp.bfloat16)


def draw_floor_gap(key, part):
    fast_head = jax.random.bernoulli(jax.random.fold_in(key, 31), 0.5, (REC_HEADS,))
    fast_channel = jnp.repeat(fast_head, REC_KEY)
    slow_rate = jnp.exp(jax.random.uniform(jax.random.fold_in(key, 32), (REC_HEADS * REC_KEY,), jnp.float32, math.log(0.5), math.log(2.0))) / SEQ_LEN
    fast_rate = jnp.exp(jax.random.uniform(jax.random.fold_in(key, 33), (REC_HEADS * REC_KEY,), jnp.float32, math.log(0.03), math.log(0.1)))
    return jnp.where(fast_channel, fast_rate, slow_rate)


def draw_decay_shift(key, part):
    dev_blocks = TOKENS // TOK_DEV
    rate_key = jax.random.fold_in(key, 41)
    rates = jnp.exp(jax.random.uniform(rate_key, (REC_HEADS, dev_blocks), jnp.float32, math.log(0.2), math.log(0.8)))
    smooth = -jnp.repeat(rates, TOK_DEV, axis=1) / SEQ_LEN
    spots = jax.random.randint(jax.random.fold_in(key, 42), (REC_HEADS, SEQS, 2), 0, SEQ_LEN)
    spots = spots + (jnp.arange(SEQS, dtype=jnp.int32) * SEQ_LEN + SEQ_LEN // 2)[None, :, None]
    drops = jnp.log(jax.random.uniform(jax.random.fold_in(key, 43), (REC_HEADS, SEQS, 2), jnp.float32, 0.5, 0.8))
    hits = jnp.arange(TOKENS, dtype=jnp.int32)[None, None, None, :] == spots[:, :, :, None]
    return smooth + jnp.sum(jnp.where(hits, drops[:, :, :, None], 0.0), axis=(1, 2))


def level_of(key, extent, shards, least, high):
    loudness, own = 1.0, jax.random.fold_in(key, 6)
    for axis_at, parts in shards:
        draws = jnp.exp(jax.random.uniform(jax.random.fold_in(own, axis_at), (parts,), jnp.float32, least / len(shards), high / len(shards)))
        loudness = loudness * jnp.repeat(draws, extent[axis_at] // parts).reshape([-1 if axis == axis_at else 1 for axis in range(len(extent))])
    return loudness


def centred(key, shape, width, reach, split=(), kind=jnp.bfloat16):
    factor_of = level_of(key, shape, split, -0.22, 0.18) if split else 1.0
    result = jax.random.normal(key, shape, jnp.float32) * width * factor_of
    return jnp.minimum(jnp.maximum(result, -reach), reach).astype(kind)


def setup_inputs(seed: int = 0) -> dict:
    key_of = jax.random.split(jax.random.key(seed), 16)
    return {
        "tokens_in": draw_tokens_in(jax.random.fold_in(key_of[15], 71), 0),
        "norm_gain": jnp.clip(1.0 + 0.18 * jax.random.normal(key_of[1], (D,), jnp.float32), 0.1, 1.9),
        "rec_query_weight": centred(key_of[2], (D, REC_HEADS * REC_KEY), D ** -0.5, 0.125, ((0, 8), (1, 4))),
        "rec_forget_weight": centred(key_of[3], (D, REC_HEADS * REC_KEY), D ** -0.5, 0.125, ((0, 8), (1, 4))),
        "rec_input_weight": centred(key_of[4], (D, REC_WIDTH), D ** -0.5, 0.125, ((0, 8), (1, 4))),
        "att_query_weight": draw_att_query_weight(jax.random.fold_in(key_of[15], 71), 0),
        "att_key_weight": draw_att_key_weight(jax.random.fold_in(key_of[15], 71), 0),
        "att_value_weight": centred(key_of[7], (D, ATT_WIDTH), D ** -0.5, 0.125, ((0, 8), (1, 4))),
        "recurrence_output_weight": centred(key_of[8], (REC_WIDTH, D), (REC_WIDTH + ATT_WIDTH) ** -0.5, 0.125, ((0, 4),)),
        "out_att_weight": centred(key_of[9], (ATT_WIDTH, D), (REC_WIDTH + ATT_WIDTH) ** -0.5, 0.125, ((0, 4),)),
        "floor_gap": draw_floor_gap(jax.random.fold_in(key_of[15], 71), 0),
        "decay_shift": draw_decay_shift(jax.random.fold_in(key_of[15], 71), 0),
        "rec_gain": jnp.clip(1.0 + 0.18 * jax.random.normal(key_of[12], (REC_VAL,), jnp.float32), 0.1, 1.9),
        "att_gain": jnp.clip(1.0 + 0.18 * jax.random.normal(key_of[13], (ATT_VAL,), jnp.float32), 0.1, 1.9),
        "lambda_head": jnp.clip(0.3 + 0.5 * jax.random.uniform(key_of[14], (ATT_HEADS,), jnp.float32) ** level_of(key_of[14], (ATT_HEADS,), ((0, 4),), -0.2, 0.2), 0.3, 0.8),
    }


RECUR_EPSILON = 1e-06
ATTEND_EPSILON = 1e-05
ROTARY_BASE = 10000.0
TOP_PRECISION = lax.Precision.HIGHEST

def rms_scale(values, scales, epsilon):
    mean_sq = lax.optimization_barrier(jnp.mean(values * values, axis=-1, keepdims=True))
    return values * lax.rsqrt(mean_sq + epsilon) * scales

def rotary(values, positions):
    half_width = values.shape[-1] // 2
    frequency = 1.0 / ROTARY_BASE ** (jnp.arange(half_width, dtype=jnp.float32) / half_width)
    angles = positions[:, None] * frequency[None, :]
    cosine = jnp.cos(angles)[:, None, :]
    sine_part = jnp.sin(angles)[:, None, :]
    first_half = values[..., :half_width]
    second_half = values[..., half_width:]
    return jnp.concatenate([first_half * cosine - second_half * sine_part, second_half * cosine + first_half * sine_part], axis=-1)

def recur_blocks(queries, gate_key_rows, inputs, log_decay, keep_flags, carry_in):
    head_count = queries.shape[0]
    length = queries.shape[1]
    block_count = length // BLOCK

    def split_blocks(array):
        return array.reshape(head_count, block_count, BLOCK, array.shape[-1]).transpose(1, 0, 2, 3)
    causal = jnp.tril(jnp.ones((BLOCK, BLOCK), dtype=bool))

    def advance(carried, bundle):
        q_block, k_block, v_block, g_block, keep_now = bundle
        carried = carried * keep_now
        cum_log = jnp.cumsum(g_block, axis=1)
        q_decayed = q_block * jnp.exp(cum_log)
        k_growth = k_block * jnp.exp(-cum_log)
        from_past = jnp.einsum('hcd,hde->hce', q_decayed, carried, precision=TOP_PRECISION)
        scores = jnp.einsum('htd,hsd->hts', q_decayed, k_growth, precision=TOP_PRECISION)
        scores = jnp.where(causal[None], scores, 0.0)
        within = jnp.einsum('hts,hse->hte', scores, v_block, precision=TOP_PRECISION)
        end_log = cum_log[:, -1:, :]
        k_to_end = k_block * jnp.exp(end_log - cum_log)
        fresh = jnp.exp(end_log[:, 0, :])[:, :, None] * carried + jnp.einsum('hsd,hse->hde', k_to_end, v_block, precision=TOP_PRECISION)
        return (fresh, from_past + within)
    final_state, outputs = lax.scan(advance, carry_in, (split_blocks(queries), split_blocks(gate_key_rows), split_blocks(inputs), split_blocks(log_decay), keep_flags))
    return (outputs.transpose(1, 0, 2, 3).reshape(head_count, length, inputs.shape[-1]), final_state)

def attend_sequence(queries, seq_keys, seq_values, segment, lambda_head):
    seq_length = queries.shape[0]
    query_rows = math.gcd(seq_length, 512)
    score_scale = queries.shape[-1] ** (-0.5)
    key_index = jnp.arange(seq_length, dtype=jnp.int32)
    keys_wide = seq_keys.astype(jnp.float32)
    values_wide = seq_values.astype(jnp.float32)

    def one_block(bundle):
        first_row, q_block, q_segment = bundle
        scores = jnp.einsum('qhcd,khcd->hcqk', q_block.astype(jnp.float32), keys_wide) * score_scale
        causal = (first_row + jnp.arange(query_rows, dtype=jnp.int32))[:, None] >= key_index[None, :]
        causal = causal & (q_segment[:, None] == segment[None, :])
        scores = jnp.where(causal, scores, -jnp.inf)
        best_score = lax.optimization_barrier(jnp.max(scores, axis=-1))
        expo_vals = jnp.exp(scores - best_score[..., None])
        totals = lax.optimization_barrier(jnp.sum(expo_vals, axis=-1))
        rounded = lax.optimization_barrier(expo_vals.astype(jnp.bfloat16)).astype(jnp.float32)
        weighted = jnp.einsum('hcqk,khe->hcqe', rounded, values_wide)
        mixed_raw = weighted[:, 0] / totals[:, 0, :, None] - lambda_head[:, None, None] * weighted[:, 1] / totals[:, 1, :, None]
        return mixed_raw.transpose(1, 0, 2)
    block_total = seq_length // query_rows
    starts = jnp.arange(block_total, dtype=jnp.int32) * query_rows
    blocks = queries.reshape(block_total, query_rows, queries.shape[1], 2, queries.shape[-1])
    return lax.map(one_block, (starts, blocks, segment.reshape(block_total, query_rows))).reshape(seq_length, queries.shape[1], seq_values.shape[-1])

def reference(tokens_in, norm_gain, rec_query_weight, rec_forget_weight, rec_input_weight, att_query_weight, att_key_weight, att_value_weight, recurrence_output_weight, out_att_weight, floor_gap, decay_shift, rec_gain, att_gain, lambda_head):
    normed = rms_scale(tokens_in.astype(jnp.float32), norm_gain, RECUR_EPSILON).astype(jnp.bfloat16)

    def project(weight):
        return jnp.dot(normed, weight, preferred_element_type=jnp.float32)
    half_seq = SEQ_LEN // 2
    token_index = jnp.arange(TOKENS, dtype=jnp.int32)
    seq_start = jnp.maximum(0, (token_index + half_seq) // SEQ_LEN * SEQ_LEN - half_seq).astype(jnp.int32)
    rec_query = project(rec_query_weight).astype(jnp.bfloat16)
    rec_forget = project(rec_forget_weight).astype(jnp.bfloat16)
    rec_input = project(rec_input_weight).astype(jnp.bfloat16)
    positions = (token_index - seq_start).astype(jnp.float32)
    att_query = rotary(project(att_query_weight).reshape(TOKENS, ATT_HEADS * 2, PAIR), positions).astype(jnp.bfloat16)
    att_key = rotary(project(att_key_weight).reshape(TOKENS, ATT_HEADS * 2, PAIR), positions).astype(jnp.bfloat16)
    att_value = project(att_value_weight).astype(jnp.bfloat16)
    gate_key = floor_gap[None, :] * jax.nn.sigmoid(-rec_forget.astype(jnp.float32))
    log_decay = jnp.log1p(-gate_key).reshape(TOKENS, REC_HEADS, REC_KEY) + decay_shift.T[:, :, None]

    def by_head(array):
        return array.reshape(TOKENS, REC_HEADS, -1).transpose(1, 0, 2)
    block_starts = jnp.arange(TOKENS // BLOCK, dtype=jnp.int32) * BLOCK
    keep_flags = jnp.where(seq_start[block_starts] == block_starts, 0.0, 1.0).astype(jnp.float32)
    rec_raw = recur_blocks(by_head(rec_query.astype(jnp.float32)), by_head(gate_key), by_head(rec_input.astype(jnp.float32)), log_decay.transpose(1, 0, 2), keep_flags, jnp.zeros((REC_HEADS, REC_KEY, REC_VAL), jnp.float32))[0]
    rec_raw = rec_raw.transpose(1, 0, 2)
    rec_mix = rms_scale(rec_raw, rec_gain, RECUR_EPSILON).astype(jnp.bfloat16).reshape(TOKENS, REC_WIDTH)

    def attend_one(bundle):
        return attend_sequence(bundle[0], bundle[1], bundle[2], bundle[3], lambda_head)
    group_count = TOKENS // SEQ_LEN
    seq_shape = (group_count, SEQ_LEN, ATT_HEADS, 2, PAIR)

    def rolled(array):
        return jnp.roll(array, -half_seq, axis=0)
    att_raw = lax.map(attend_one, (rolled(att_query).reshape(seq_shape), rolled(att_key).reshape(seq_shape), rolled(att_value).reshape(group_count, SEQ_LEN, ATT_HEADS, ATT_VAL), rolled(seq_start).reshape(group_count, SEQ_LEN)))
    att_raw = jnp.roll(att_raw.reshape(TOKENS, ATT_HEADS, ATT_VAL), half_seq, axis=0)
    att_mix = rms_scale(att_raw, att_gain, ATTEND_EPSILON).astype(jnp.bfloat16).reshape(TOKENS, ATT_WIDTH)
    rec_rows = REC_WIDTH // N_TP
    att_rows = ATT_WIDTH // N_TP
    summed = jnp.zeros((TOKENS, D), jnp.float32)
    for group in range(N_TP):
        partial_value = jnp.dot(rec_mix[:, group * rec_rows:(group + 1) * rec_rows], recurrence_output_weight[group * rec_rows:(group + 1) * rec_rows], preferred_element_type=jnp.float32)
        partial_value = partial_value + jnp.dot(att_mix[:, group * att_rows:(group + 1) * att_rows], out_att_weight[group * att_rows:(group + 1) * att_rows], preferred_element_type=jnp.float32)
        summed = summed + lax.optimization_barrier(partial_value.astype(jnp.bfloat16)).astype(jnp.float32)
    return summed.astype(jnp.bfloat16)
```

```python
import functools

import jax
import jax.numpy as jnp
from jax import lax
from jax.experimental import pallas as pl
from jax.experimental.pallas import tpu as pltpu
from jax.sharding import PartitionSpec as P

REC_KEY = 128
REC_VAL = 128
PAIR = 64
ATT_VAL = 128
BLOCK = 64


RECUR_EPSILON = 1e-06
ATTEND_EPSILON = 1e-05
ROTARY_BASE = 10000.0
TOP_PRECISION = lax.Precision.HIGHEST


def prefix_2(array, axis, combine, identity):
    count, position = (lax.axis_size(axis), lax.axis_index(axis))
    everything = jax.tree.map(
        lambda part, kind: lax.all_gather(part.astype(kind), axis),
        array,
        (jnp.bfloat16, jnp.bfloat16),
    )
    start = jax.tree.map(
        lambda part, zero: jnp.broadcast_to(jnp.asarray(zero, part.dtype), part.shape),
        array,
        identity,
    )

    def turn(k, before):
        reached = k < position
        new = combine(
            before, jax.tree.map(lambda part, own: part[k].astype(own.dtype), everything, array)
        )
        return jax.tree.map(lambda a, b: jnp.where(reached, a, b), new, before)

    return lax.fori_loop(0, count, turn, start)


def from_behind(block, axis, distance):
    devices = range(lax.axis_size(axis))
    route = [(i - distance, i) for i in devices if i - distance in devices]
    return lax.ppermute(block, axis, route)


def rms_scale(values, scales, epsilon):
    mean_sq = jnp.mean(values * values, axis=-1, keepdims=True)
    return values * lax.rsqrt(mean_sq + epsilon) * scales


def rotary(values, positions):
    half_width = values.shape[-1] // 2
    frequency = 1.0 / ROTARY_BASE ** (jnp.arange(half_width, dtype=jnp.float32) / half_width)
    angles = positions[:, None] * frequency[None, :]
    cosine = jnp.cos(angles)[:, None, :]
    sine_part = jnp.sin(angles)[:, None, :]
    first_half = values[..., :half_width]
    second_half = values[..., half_width:]
    return jnp.concatenate(
        [
            first_half * cosine - second_half * sine_part,
            second_half * cosine + first_half * sine_part,
        ],
        axis=-1,
    )


def recur_blocks(queries, gate_key_rows, inputs, log_decay, carry_in):
    head_count = queries.shape[0]
    length = queries.shape[1]
    block_count = length // BLOCK

    def split_blocks(array):
        return array.reshape(head_count, block_count, BLOCK, array.shape[-1]).transpose(1, 0, 2, 3)

    causal = jnp.tril(jnp.ones((BLOCK, BLOCK), dtype=bool))

    def advance(carried, bundle):
        q_block, k_block, v_block, g_block = bundle
        cum_log = jnp.cumsum(g_block, axis=1)
        q_decayed = q_block * jnp.exp(cum_log)
        k_growth = k_block * jnp.exp(-cum_log)
        from_past = jnp.einsum("hcd,hde->hce", q_decayed, carried, precision=TOP_PRECISION)
        scores = jnp.einsum("htd,hsd->hts", q_decayed, k_growth, precision=TOP_PRECISION)
        scores = jnp.where(causal[None], scores, 0.0)
        within = jnp.einsum("hts,hse->hte", scores, v_block, precision=TOP_PRECISION)
        end_log = cum_log[:, -1:, :]
        k_to_end = k_block * jnp.exp(end_log - cum_log)
        fresh = jnp.exp(end_log[:, 0, :])[:, :, None] * carried + jnp.einsum(
            "hsd,hse->hde", k_to_end, v_block, precision=TOP_PRECISION
        )
        return (fresh, from_past + within)

    final_state, outputs = lax.scan(
        advance,
        carry_in,
        (
            split_blocks(queries),
            split_blocks(gate_key_rows),
            split_blocks(inputs),
            split_blocks(log_decay),
        ),
    )
    return (
        outputs.transpose(1, 0, 2, 3).reshape(head_count, length, inputs.shape[-1]),
        final_state,
    )


def chain(earlier, latter):
    return (earlier[0] * latter[0], latter[0][:, :, None] * earlier[1] + latter[1])


def absorb(running_total, queries, key_rows, value_rows, allowed):
    best_score, sums_exp, weighted = running_total
    scores = jnp.einsum(
        "qhcd,khcd->hcqk", queries, key_rows, preferred_element_type=jnp.float32
    ) * queries.shape[-1] ** (-0.5)
    scores = jnp.where(allowed, scores, -jnp.inf)
    new_best = jnp.maximum(best_score, jnp.max(scores, axis=-1))
    rescale = jnp.exp(best_score - new_best)
    expo_vals = jnp.exp(scores - new_best[..., None])
    sums_exp = sums_exp * rescale + jnp.sum(expo_vals, axis=-1)
    weighted = weighted * rescale[..., None] + jnp.einsum(
        "hcqk,khe->hcqe",
        expo_vals.astype(jnp.bfloat16),
        value_rows,
        preferred_element_type=jnp.float32,
    )
    return (new_best, sums_exp, weighted)


def per_device(
    tokens_in,
    norm_gain,
    rec_query_weight,
    rec_forget_weight,
    rec_input_weight,
    att_query_weight,
    att_key_weight,
    att_value_weight,
    recurrence_output_weight,
    out_att_weight,
    floor_gap,
    decay_shift,
    rec_gain,
    att_gain,
    lambda_head,
):
    tok_rows = tokens_in.shape[0]
    seq_span = lax.axis_size("sp") // 4
    half_span = seq_span // 2
    dev_index = lax.axis_index("sp")
    first_dev = jnp.maximum(0, (dev_index + half_span) // seq_span * seq_span - half_span)
    carry_on = jnp.where(dev_index == first_dev, 0.0, 1.0).astype(jnp.float32)
    gathered = (
        lax.all_gather(rec_query_weight, "sp", axis=0, tiled=True),
        lax.all_gather(rec_forget_weight, "sp", axis=0, tiled=True),
        lax.all_gather(rec_input_weight, "sp", axis=0, tiled=True),
        lax.all_gather(att_query_weight, "sp", axis=0, tiled=True),
        lax.all_gather(att_key_weight, "sp", axis=0, tiled=True),
        lax.all_gather(att_value_weight, "sp", axis=0, tiled=True),
    )
    w_query, w_forget, w_input, w_att_query, w_att_key, w_att_value = gathered
    normed = rms_scale(tokens_in.astype(jnp.float32), norm_gain, RECUR_EPSILON).astype(jnp.bfloat16)

    def project(weight):
        return jnp.dot(normed, weight, preferred_element_type=jnp.float32)

    rec_query = project(w_query).astype(jnp.bfloat16)
    rec_forget = project(w_forget).astype(jnp.bfloat16)
    rec_input = project(w_input).astype(jnp.bfloat16)
    att_heads = w_att_query.shape[1] // (2 * PAIR)
    positions = ((dev_index - first_dev) * tok_rows + jnp.arange(tok_rows, dtype=jnp.int32)).astype(
        jnp.float32
    )
    att_query = (
        rotary(project(w_att_query).reshape(tok_rows, att_heads * 2, PAIR), positions)
        .astype(jnp.bfloat16)
        .reshape(tok_rows, att_heads, 2, PAIR)
    )
    att_key = (
        rotary(project(w_att_key).reshape(tok_rows, att_heads * 2, PAIR), positions)
        .astype(jnp.bfloat16)
        .reshape(tok_rows, att_heads * 2 * PAIR)
    )
    att_value = project(w_att_value).astype(jnp.bfloat16)
    rec_heads = w_query.shape[1] // REC_KEY
    gate_key = floor_gap[None, :] * jax.nn.sigmoid(-rec_forget.astype(jnp.float32))
    log_decay = (
        jnp.log1p(-gate_key).reshape(tok_rows, rec_heads, REC_KEY) + decay_shift.T[:, :, None]
    )

    def by_head(array, column_count):
        return array.reshape(tok_rows, rec_heads, column_count).transpose(1, 0, 2)

    query_heads = by_head(rec_query.astype(jnp.float32), REC_KEY)
    k_heads = by_head(gate_key, REC_KEY)
    v_heads = by_head(rec_input.astype(jnp.float32), REC_VAL)
    g_heads = log_decay.transpose(1, 0, 2)
    zero_state = jnp.zeros((rec_heads, REC_KEY, REC_VAL), jnp.float32)
    local_out, local_state = recur_blocks(query_heads, k_heads, v_heads, g_heads, zero_state)
    reach_logarithm = jnp.cumsum(g_heads, axis=1)
    span_decay = jnp.exp(reach_logarithm[:, -1, :]) * carry_on
    prefix = prefix_2(
        (span_decay, local_state), "sp", chain, (jnp.ones_like(span_decay), zero_state)
    )
    incoming_state = prefix[1] * carry_on
    rec_raw = local_out + jnp.einsum(
        "ezp,ept->ezt",
        query_heads * jnp.exp(reach_logarithm),
        incoming_state,
        precision=TOP_PRECISION,
    )
    rec_mix = (
        rms_scale(rec_raw.transpose(1, 0, 2), rec_gain, RECUR_EPSILON)
        .astype(jnp.bfloat16)
        .reshape(tok_rows, rec_heads * REC_VAL)
    )
    mask_own = jnp.arange(tok_rows)[:, None] >= jnp.arange(tok_rows)[None, :]
    start_state = (
        jnp.full((att_heads, 2, tok_rows), -jnp.inf, jnp.float32),
        jnp.zeros((att_heads, 2, tok_rows), jnp.float32),
        jnp.zeros((att_heads, 2, tok_rows, ATT_VAL), jnp.float32),
    )
    online = absorb(
        start_state,
        att_query,
        att_key.reshape(tok_rows, att_heads, 2, PAIR),
        att_value.reshape(tok_rows, att_heads, ATT_VAL),
        mask_own,
    )
    everything = jnp.array(True)

    def take_block(state_now, keys_flat, values_flat, source):
        key_rows = keys_flat.reshape(tok_rows, att_heads, 2, PAIR)
        value_rows = values_flat.reshape(tok_rows, att_heads, ATT_VAL)
        return lax.cond(
            source >= first_dev,
            lambda held: absorb(held, att_query, key_rows, value_rows, everything),
            lambda held: held,
            state_now,
        )

    def relay_turn(hop_count, carried):
        moving_keys, moving_values, state_now = carried
        moving_keys, moving_values = from_behind((moving_keys, moving_values), "sp", 1)
        return (
            moving_keys,
            moving_values,
            take_block(state_now, moving_keys, moving_values, dev_index - hop_count - 1),
        )

    online = lax.fori_loop(0, seq_span - 1, relay_turn, (att_key, att_value, online))[2]
    best_score, sums_exp, weighted = online
    att_raw = (
        weighted[:, 0] / sums_exp[:, 0, :, None]
        - lambda_head[:, None, None] * weighted[:, 1] / sums_exp[:, 1, :, None]
    )
    att_mix = (
        rms_scale(att_raw.transpose(1, 0, 2), att_gain, ATTEND_EPSILON)
        .astype(jnp.bfloat16)
        .reshape(tok_rows, att_heads * ATT_VAL)
    )
    partial_value = jnp.dot(rec_mix, recurrence_output_weight, preferred_element_type=jnp.float32)
    partial_value = partial_value + jnp.dot(
        att_mix, out_att_weight, preferred_element_type=jnp.float32
    )
    return lax.psum(partial_value.astype(jnp.bfloat16), "tp")


MESH = pl.DeviceIdType.MESH
F32 = jnp.float32
BF16 = jnp.bfloat16
CUT = 128


def nt(a, b):
    return lax.dot_general(a, b, (((1,), (1,)), ((), ())), preferred_element_type=F32)


def tn(a, b):
    return lax.dot_general(a, b, (((0,), (0,)), ((), ())), preferred_element_type=F32)


def nn(a, b):
    return jnp.dot(a, b, preferred_element_type=F32)


def halves(x):
    high = x.astype(BF16)
    return high, (x - high.astype(F32)).astype(BF16)


def turn_map(values, cosine, sine_part):
    width = values.shape[-1]
    lane = lax.broadcasted_iota(jnp.int32, values.shape, 1)
    ahead = pltpu.roll(values, width - PAIR // 2, 1)
    back = pltpu.roll(values, PAIR // 2, 1)
    other = jnp.where(lane % PAIR < PAIR // 2, ahead, back)
    return values * cosine + other * sine_part


def fused_kernel(
    n, tps, span,
    tokens, gain, wk, wv, wq, wf, wi, wr, rec_out, att_out, gap, shift, rec_gain, att_gain, cosine, sine_part,
    lam, out,
    buf, xn, acc, wo, mix, kv, kv_prev, st, st_prev, total,
    ssem, rsem, wo_s, wo_r, mix_s, mix_r, ex_s, ex_r,
):
    weights = (wk, wv, wq, wf, wi, wr)
    chunks = len(weights)
    rows, width = tokens.shape
    depth, cols = wk.shape
    me = lax.axis_index("sp")
    t = lax.axis_index("tp")
    up = (1 - me % 2)
    place = up * (me // 2) + (1 - up) * (n - 1 - me // 2)

    def at_place(p):
        q = (p + n) % n
        low = q // (n // 2)
        return (1 - low) * (2 * q) + low * (2 * (n - 1 - q) + 1)

    right, left = at_place(place + 1), at_place(place - 1)
    partner = t + 1 - 2 * (t % 2)
    across = (t + 2) % tps
    half = span // 2
    stage = (me + half) % span
    is_recv = jnp.logical_and(stage > 0, me >= half)
    is_send = jnp.logical_and(stage == 0, me + 1 < n)
    to_right, to_left = {"sp": right}, {"sp": left}
    to_partner, to_across = {"tp": partner}, {"tp": across}

    barrier = pltpu.get_barrier_semaphore()
    for target in (to_right, to_left, to_partner, to_across):
        pl.semaphore_signal(barrier, inc=1, device_id=target, device_id_type=MESH)

    @pl.when(is_send)
    def _():
        pl.semaphore_signal(barrier, inc=1, device_id={"sp": me + 1}, device_id_type=MESH)

    @pl.when(is_recv)
    def _():
        pl.semaphore_signal(barrier, inc=1, device_id={"sp": me - 1}, device_id_type=MESH)

    paired = jnp.logical_or(is_send, is_recv)

    @pl.when(paired)
    def _():
        pl.semaphore_wait(barrier, 5)

    @pl.when(jnp.logical_not(paired))
    def _():
        pl.semaphore_wait(barrier, 4)

    top = n // 2

    def slot(way, hop):
        return hop if way == 0 else n - hop

    def carried(way, hop):
        if hop < top:
            return tuple(range(chunks))
        if hop == top:
            return tuple(range(chunks // 2)) if way == 0 else tuple(range(chunks // 2, chunks))
        return ()

    def ring(way, hop, c):
        return pltpu.make_async_remote_copy(
            src_ref=weights[c] if hop == 1 else buf.at[slot(way, hop - 1), c],
            dst_ref=buf.at[slot(way, hop), c],
            send_sem=ssem.at[way, hop - 1, c],
            recv_sem=rsem.at[slot(way, hop), c],
            device_id=(to_right, to_left)[way],
            device_id_type=MESH,
        )

    def remote(src, dst, s, r, target):
        return pltpu.make_async_remote_copy(
            src_ref=src, dst_ref=dst, send_sem=s, recv_sem=r, device_id=target, device_id_type=MESH
        )

    outs_w = (rec_out, att_out)

    def wo_copy(k, part):
        src = outs_w[part] if k < 2 else wo.at[1, part]
        return remote(src, wo.at[k, part], wo_s.at[k, part], wo_r.at[k, part], to_across if k == 1 else to_partner)

    def mix_copy(k, part):
        src = mix.at[3, part] if k < 2 else mix.at[1, part]
        return remote(src, mix.at[k, part], mix_s.at[k, part], mix_r.at[k, part], to_across if k == 1 else to_partner)

    for c in range(chunks):
        for way in range(2):
            ring(way, 1, c).start()
    for part in range(2):
        wo_copy(1, part).start()
        wo_copy(0, part).start()

    values = tokens[...].astype(F32)
    mean_sq = jnp.mean(values * values, axis=-1, keepdims=True)
    normed = (values * lax.rsqrt(mean_sq + RECUR_EPSILON) * gain[...]).astype(BF16)
    for k in range(n):
        xn[k] = normed[:, k * depth : (k + 1) * depth]
    mine = xn[me]
    for c in range(chunks):
        acc[c] = nn(mine, weights[c][...])

    def project(way, hop, c):
        ring(way, hop, c).wait_recv()
        if c in carried(way, hop + 1):
            ring(way, hop + 1, c).start()
        origin = at_place(place - hop if way == 0 else place + hop)
        acc[c] = acc[c] + nn(xn[origin], buf[slot(way, hop), c])

    for hop in range(1, top):
        for c in range(chunks):
            for way in range(2):
                project(way, hop, c)
    for part in range(2):
        wo_copy(1, part).wait_recv()
        wo_copy(2, part).start()

    @pl.when(jnp.logical_not(is_recv))
    def _():
        kv_prev[...] = jnp.zeros(kv_prev.shape, BF16)
        st_prev[...] = jnp.zeros(st_prev.shape, F32)

    def ex_copy(k):
        src, dst = ((kv.at[0], kv_prev.at[0]), (kv.at[1], kv_prev.at[1]), (st, st_prev))[k]
        return remote(src, dst, ex_s.at[k], ex_r.at[k], {"sp": me + 1})

    heads = cols // CUT
    blocks = rows // CUT
    r_iota = lax.broadcasted_iota(jnp.int32, (CUT, CUT), 0)
    c_iota = lax.broadcasted_iota(jnp.int32, (CUT, CUT), 1)
    lower = r_iota >= c_iota
    ones = jnp.where(lower, 1.0, 0.0).astype(BF16)

    project(0, top, 0)
    for h in range(heads):
        lanes = slice(h * CUT, (h + 1) * CUT)
        kv[0, :, lanes] = turn_map(acc[0, :, lanes], cosine[...], sine_part[...]).astype(BF16)

    @pl.when(is_send)
    def _():
        ex_copy(0).start()

    project(1, top, 3)
    cums, keys = [], []
    for h in range(heads):
        lanes = slice(h * CUT, (h + 1) * CUT)
        forget = acc[3, :, lanes].astype(BF16).astype(F32)
        key = gap[:, lanes] * (1.0 / (1.0 + jnp.exp(forget)))
        high, low = halves(jnp.log(1.0 - key))
        for b in range(blocks):
            part = slice(b * CUT, (b + 1) * CUT)
            s_high, s_low = halves(jnp.broadcast_to(shift[h : h + 1, part], (CUT, CUT)))
            cums.append(nn(ones, high[part]) + nn(ones, low[part]) + nt(ones, s_high) + nt(ones, s_low))
            keys.append(key[part])

    project(0, top, 1)
    kv[1] = acc[1].astype(BF16)

    @pl.when(is_send)
    def _():
        ex_copy(1).start()

    project(1, top, 4)
    fresh, inputs = [], []
    for h in range(heads):
        lanes = slice(h * CUT, (h + 1) * CUT)
        own = jnp.zeros((CUT, CUT), F32)
        for b in range(blocks):
            i = h * blocks + b
            inp = acc[4, b * CUT : (b + 1) * CUT, lanes].astype(BF16)
            end = cums[i][CUT - 1 : CUT]
            to_end = (keys[i] * jnp.exp(end - cums[i])).astype(BF16)
            fresh.append(own)
            own = own * jnp.exp(end) + tn(inp, to_end)
            inputs.append(inp)
        st[h] = own

    @pl.when(is_send)
    def _():
        ex_copy(2).start()

    project(0, top, 2)
    project(1, top, 5)

    raws, pasts = [], []
    for h in range(heads):
        lanes = slice(h * CUT, (h + 1) * CUT)
        decay = jnp.zeros((1, CUT), F32)
        for b in range(blocks):
            i = h * blocks + b
            cum = cums[i]
            middle = cum[CUT // 2 - 1 : CUT // 2]
            q = acc[5, b * CUT : (b + 1) * CUT, lanes].astype(BF16).astype(F32)
            scores = nt((q * jnp.exp(cum - middle)).astype(BF16), (keys[i] * jnp.exp(middle - cum)).astype(BF16))
            scores = jnp.where(lower, scores, 0.0).astype(BF16)
            past = q * jnp.exp(cum)
            raw = nn(scores, inputs[i])
            if b:
                raw = raw + nt(past.astype(BF16), fresh[i].astype(BF16))
            raws.append(raw)
            pasts.append((past, decay))
            decay = decay + cum[CUT - 1 : CUT]

    for part in range(2):
        wo_copy(0, part).wait_recv()
        wo_copy(2, part).wait_recv()

    lane = lax.broadcasted_iota(jnp.int32, (rows, CUT), 1)
    own_mask = lax.broadcasted_iota(jnp.int32, (rows, rows), 0) >= lax.broadcasted_iota(jnp.int32, (rows, rows), 1)
    away = jnp.where(is_recv, 0.0, -1e30).astype(F32)

    own_scores = []
    turned = []
    for h in range(heads):
        lanes = slice(h * CUT, (h + 1) * CUT)
        query = turn_map(acc[2, :, lanes], cosine[...], sine_part[...]).astype(BF16)
        for c in range(2):
            picked = jnp.where((lane // PAIR) == c, query, jnp.zeros_like(query))
            turned.append(picked)

    @pl.when(is_recv)
    def _():
        for k in range(3):
            ex_copy(k).wait_recv()

    for h in range(heads):
        lanes = slice(h * CUT, (h + 1) * CUT)
        for b in range(blocks):
            i = h * blocks + b
            past, decay = pasts[i]
            came = (st_prev[h] * jnp.exp(decay)).astype(BF16)
            raw = raws[i] + nt(past.astype(BF16), came)
            mean_sq = jnp.mean(raw * raw, axis=-1, keepdims=True)
            mix[3, 0, b * CUT : (b + 1) * CUT, lanes] = (
                raw * lax.rsqrt(mean_sq + RECUR_EPSILON) * rec_gain[...]
            ).astype(BF16)
    mix_copy(1, 0).start()
    mix_copy(0, 0).start()

    for h in range(heads):
        lanes = slice(h * CUT, (h + 1) * CUT)
        found = []
        for c in range(2):
            picked = turned[h * 2 + c]
            s_own = jnp.where(own_mask, nt(picked, kv[0, :, lanes]) * PAIR ** (-0.5), -1e30)
            s_prev = nt(picked, kv_prev[0, :, lanes]) * PAIR ** (-0.5) + away
            best = jnp.maximum(jnp.max(s_own, axis=-1, keepdims=True), jnp.max(s_prev, axis=-1, keepdims=True))
            e_own, e_prev = jnp.exp(s_own - best), jnp.exp(s_prev - best)
            sums = jnp.sum(e_own, axis=-1, keepdims=True) + jnp.sum(e_prev, axis=-1, keepdims=True)
            weighted = nn(e_own.astype(BF16), kv[1, :, lanes]) + nn(e_prev.astype(BF16), kv_prev[1, :, lanes])
            found.append(weighted / sums)
        raw = found[0] - lam[h] * found[1]
        mean_sq = jnp.mean(raw * raw, axis=-1, keepdims=True)
        mix[3, 1, :, lanes] = (raw * lax.rsqrt(mean_sq + ATTEND_EPSILON) * att_gain[...]).astype(BF16)
    mix_copy(1, 1).start()
    mix_copy(0, 1).start()

    tile = 2 * cols
    tiles = width // tile

    def add(k, part, first=False):
        source = outs_w[part] if k == 3 else wo.at[k, part]
        left_side = mix[k, part]
        for j in range(tiles):
            span_cols = slice(j * tile, (j + 1) * tile)
            product = nn(left_side, source[:, span_cols])
            total[:, span_cols] = product if first else total[:, span_cols] + product

    add(3, 0, True)
    mix_copy(1, 0).wait_recv()
    mix_copy(2, 0).start()
    add(3, 1)
    mix_copy(0, 0).wait_recv()
    add(0, 0)
    add(1, 0)
    mix_copy(2, 0).wait_recv()
    add(2, 0)
    mix_copy(0, 1).wait_recv()
    add(0, 1)
    mix_copy(1, 1).wait_recv()
    mix_copy(2, 1).start()
    add(1, 1)
    mix_copy(2, 1).wait_recv()
    left_side = mix[2, 1]
    for j in range(tiles):
        span_cols = slice(j * tile, (j + 1) * tile)
        out[:, span_cols] = (total[:, span_cols] + nn(left_side, wo[2, 1, :, span_cols])).astype(BF16)

    for hop in range(1, top + 1):
        for way in range(2):
            for c in carried(way, hop):
                ring(way, hop, c).wait_send()
    for k in range(3):
        for part in range(2):
            wo_copy(k, part).wait_send()
            mix_copy(k, part).wait_send()

    @pl.when(is_send)
    def _():
        for k in range(3):
            ex_copy(k).wait_send()


def per_device_fused(
    n, tps, span,
    tokens_in, norm_gain, rec_query_weight, rec_forget_weight, rec_input_weight,
    att_query_weight, att_key_weight, att_value_weight, recurrence_output_weight, out_att_weight,
    floor_gap, decay_shift, rec_gain, att_gain, lambda_head,
):
    rows, width = tokens_in.shape
    depth, cols = att_key_weight.shape
    me = lax.axis_index("sp")
    half = span // 2
    first_dev = jnp.maximum(0, (me + half) // span * span - half)
    positions = ((me - first_dev) * rows + jnp.arange(rows, dtype=jnp.int32)).astype(F32)
    half_width = PAIR // 2
    frequency = 1.0 / ROTARY_BASE ** (jnp.arange(half_width, dtype=F32) / half_width)
    angles = positions[:, None] * frequency[None, :]
    cosine = jnp.tile(jnp.cos(angles), (1, 4))
    sine_one = jnp.sin(angles)
    sine_part = jnp.concatenate([-sine_one, sine_one, -sine_one, sine_one], axis=1)
    heads = cols // CUT
    vmem = pl.BlockSpec(memory_space=pltpu.VMEM)
    return pl.pallas_call(
        functools.partial(fused_kernel, n, tps, span),
        out_shape=jax.ShapeDtypeStruct((rows, width), BF16),
        in_specs=[vmem] * 16 + [pl.BlockSpec(memory_space=pltpu.SMEM)],
        out_specs=vmem,
        scratch_shapes=[
            pltpu.VMEM((n, 6, depth, cols), BF16),
            pltpu.VMEM((n, rows, depth), BF16),
            pltpu.VMEM((6, rows, cols), F32),
            pltpu.VMEM((3, 2, cols, width), BF16),
            pltpu.VMEM((4, 2, rows, cols), BF16),
            pltpu.VMEM((2, rows, cols), BF16),
            pltpu.VMEM((2, rows, cols), BF16),
            pltpu.VMEM((heads, CUT, CUT), F32),
            pltpu.VMEM((heads, CUT, CUT), F32),
            pltpu.VMEM((rows, width), F32),
            pltpu.SemaphoreType.DMA((2, n // 2, 6)),
            pltpu.SemaphoreType.DMA((n, 6)),
            pltpu.SemaphoreType.DMA((3, 2)),
            pltpu.SemaphoreType.DMA((3, 2)),
            pltpu.SemaphoreType.DMA((3, 2)),
            pltpu.SemaphoreType.DMA((3, 2)),
            pltpu.SemaphoreType.DMA((3,)),
            pltpu.SemaphoreType.DMA((3,)),
        ],
        compiler_params=pltpu.CompilerParams(collective_id=0, has_side_effects=True, vmem_limit_bytes=56 << 20),
    )(
        tokens_in, norm_gain[None], att_key_weight, att_value_weight, att_query_weight,
        rec_forget_weight, rec_input_weight, rec_query_weight, recurrence_output_weight, out_att_weight,
        floor_gap[None], decay_shift, rec_gain[None], att_gain[None], cosine, sine_part, lambda_head,
    )


def solution(mesh):
    in_specs = (
        P("sp", None),
        P(),
        P("sp", "tp"),
        P("sp", "tp"),
        P("sp", "tp"),
        P("sp", "tp"),
        P("sp", "tp"),
        P("sp", "tp"),
        P("tp", None),
        P("tp", None),
        P("tp"),
        P("tp", "sp"),
        P(),
        P(),
        P("tp"),
    )
    out_specs = P("sp", None)
    n, tps = mesh.shape["sp"], mesh.shape["tp"]
    span = n // 4
    chosen = per_device
    if span == 2 and tps == 4:
        chosen = functools.partial(per_device_fused, n, tps, span)
    return jax.shard_map(
        chosen, mesh=mesh, in_specs=in_specs, out_specs=out_specs, check_vma=False
    )
```

```python
import functools

import jax
import jax.numpy as jnp
from jax import lax
from jax.experimental import pallas as pl
from jax.experimental.pallas import tpu as pltpu
from jax.sharding import PartitionSpec as P

REC_KEY = 128
REC_VAL = 128
PAIR = 64
ATT_VAL = 128
BLOCK = 64


RECUR_EPSILON = 1e-06
ATTEND_EPSILON = 1e-05
ROTARY_BASE = 10000.0
TOP_PRECISION = lax.Precision.HIGHEST


def prefix_2(array, axis, combine, identity):
    count, position = (lax.axis_size(axis), lax.axis_index(axis))
    everything = jax.tree.map(
        lambda part, kind: lax.all_gather(part.astype(kind), axis),
        array,
        (jnp.bfloat16, jnp.bfloat16),
    )
    start = jax.tree.map(
        lambda part, zero: jnp.broadcast_to(jnp.asarray(zero, part.dtype), part.shape),
        array,
        identity,
    )

    def turn(k, before):
        reached = k < position
        new = combine(
            before, jax.tree.map(lambda part, own: part[k].astype(own.dtype), everything, array)
        )
        return jax.tree.map(lambda a, b: jnp.where(reached, a, b), new, before)

    return lax.fori_loop(0, count, turn, start)


def from_behind(block, axis, distance):
    devices = range(lax.axis_size(axis))
    route = [(i - distance, i) for i in devices if i - distance in devices]
    return lax.ppermute(block, axis, route)


def rms_scale(values, scales, epsilon):
    mean_sq = jnp.mean(values * values, axis=-1, keepdims=True)
    return values * lax.rsqrt(mean_sq + epsilon) * scales


def rotary(values, positions):
    half_width = values.shape[-1] // 2
    frequency = 1.0 / ROTARY_BASE ** (jnp.arange(half_width, dtype=jnp.float32) / half_width)
    angles = positions[:, None] * frequency[None, :]
    cosine = jnp.cos(angles)[:, None, :]
    sine_part = jnp.sin(angles)[:, None, :]
    first_half = values[..., :half_width]
    second_half = values[..., half_width:]
    return jnp.concatenate(
        [
            first_half * cosine - second_half * sine_part,
            second_half * cosine + first_half * sine_part,
        ],
        axis=-1,
    )


def recur_blocks(queries, gate_key_rows, inputs, log_decay, carry_in):
    head_count = queries.shape[0]
    length = queries.shape[1]
    block_count = length // BLOCK

    def split_blocks(array):
        return array.reshape(head_count, block_count, BLOCK, array.shape[-1]).transpose(1, 0, 2, 3)

    causal = jnp.tril(jnp.ones((BLOCK, BLOCK), dtype=bool))

    def advance(carried, bundle):
        q_block, k_block, v_block, g_block = bundle
        cum_log = jnp.cumsum(g_block, axis=1)
        q_decayed = q_block * jnp.exp(cum_log)
        k_growth = k_block * jnp.exp(-cum_log)
        from_past = jnp.einsum("hcd,hde->hce", q_decayed, carried, precision=TOP_PRECISION)
        scores = jnp.einsum("htd,hsd->hts", q_decayed, k_growth, precision=TOP_PRECISION)
        scores = jnp.where(causal[None], scores, 0.0)
        within = jnp.einsum("hts,hse->hte", scores, v_block, precision=TOP_PRECISION)
        end_log = cum_log[:, -1:, :]
        k_to_end = k_block * jnp.exp(end_log - cum_log)
        fresh = jnp.exp(end_log[:, 0, :])[:, :, None] * carried + jnp.einsum(
            "hsd,hse->hde", k_to_end, v_block, precision=TOP_PRECISION
        )
        return (fresh, from_past + within)

    final_state, outputs = lax.scan(
        advance,
        carry_in,
        (
            split_blocks(queries),
            split_blocks(gate_key_rows),
            split_blocks(inputs),
            split_blocks(log_decay),
        ),
    )
    return (
        outputs.transpose(1, 0, 2, 3).reshape(head_count, length, inputs.shape[-1]),
        final_state,
    )


def chain(earlier, latter):
    return (earlier[0] * latter[0], latter[0][:, :, None] * earlier[1] + latter[1])


def absorb(running_total, queries, key_rows, value_rows, allowed):
    best_score, sums_exp, weighted = running_total
    scores = jnp.einsum(
        "qhcd,khcd->hcqk", queries, key_rows, preferred_element_type=jnp.float32
    ) * queries.shape[-1] ** (-0.5)
    scores = jnp.where(allowed, scores, -jnp.inf)
    new_best = jnp.maximum(best_score, jnp.max(scores, axis=-1))
    rescale = jnp.exp(best_score - new_best)
    expo_vals = jnp.exp(scores - new_best[..., None])
    sums_exp = sums_exp * rescale + jnp.sum(expo_vals, axis=-1)
    weighted = weighted * rescale[..., None] + jnp.einsum(
        "hcqk,khe->hcqe",
        expo_vals.astype(jnp.bfloat16),
        value_rows,
        preferred_element_type=jnp.float32,
    )
    return (new_best, sums_exp, weighted)


def per_device(
    tokens_in,
    norm_gain,
    rec_query_weight,
    rec_forget_weight,
    rec_input_weight,
    att_query_weight,
    att_key_weight,
    att_value_weight,
    recurrence_output_weight,
    out_att_weight,
    floor_gap,
    decay_shift,
    rec_gain,
    att_gain,
    lambda_head,
):
    tok_rows = tokens_in.shape[0]
    seq_span = lax.axis_size("sp") // 4
    half_span = seq_span // 2
    dev_index = lax.axis_index("sp")
    first_dev = jnp.maximum(0, (dev_index + half_span) // seq_span * seq_span - half_span)
    carry_on = jnp.where(dev_index == first_dev, 0.0, 1.0).astype(jnp.float32)
    gathered = (
        lax.all_gather(rec_query_weight, "sp", axis=0, tiled=True),
        lax.all_gather(rec_forget_weight, "sp", axis=0, tiled=True),
        lax.all_gather(rec_input_weight, "sp", axis=0, tiled=True),
        lax.all_gather(att_query_weight, "sp", axis=0, tiled=True),
        lax.all_gather(att_key_weight, "sp", axis=0, tiled=True),
        lax.all_gather(att_value_weight, "sp", axis=0, tiled=True),
    )
    w_query, w_forget, w_input, w_att_query, w_att_key, w_att_value = gathered
    normed = rms_scale(tokens_in.astype(jnp.float32), norm_gain, RECUR_EPSILON).astype(jnp.bfloat16)

    def project(weight):
        return jnp.dot(normed, weight, preferred_element_type=jnp.float32)

    rec_query = project(w_query).astype(jnp.bfloat16)
    rec_forget = project(w_forget).astype(jnp.bfloat16)
    rec_input = project(w_input).astype(jnp.bfloat16)
    att_heads = w_att_query.shape[1] // (2 * PAIR)
    positions = ((dev_index - first_dev) * tok_rows + jnp.arange(tok_rows, dtype=jnp.int32)).astype(
        jnp.float32
    )
    att_query = (
        rotary(project(w_att_query).reshape(tok_rows, att_heads * 2, PAIR), positions)
        .astype(jnp.bfloat16)
        .reshape(tok_rows, att_heads, 2, PAIR)
    )
    att_key = (
        rotary(project(w_att_key).reshape(tok_rows, att_heads * 2, PAIR), positions)
        .astype(jnp.bfloat16)
        .reshape(tok_rows, att_heads * 2 * PAIR)
    )
    att_value = project(w_att_value).astype(jnp.bfloat16)
    rec_heads = w_query.shape[1] // REC_KEY
    gate_key = floor_gap[None, :] * jax.nn.sigmoid(-rec_forget.astype(jnp.float32))
    log_decay = (
        jnp.log1p(-gate_key).reshape(tok_rows, rec_heads, REC_KEY) + decay_shift.T[:, :, None]
    )

    def by_head(array, column_count):
        return array.reshape(tok_rows, rec_heads, column_count).transpose(1, 0, 2)

    query_heads = by_head(rec_query.astype(jnp.float32), REC_KEY)
    k_heads = by_head(gate_key, REC_KEY)
    v_heads = by_head(rec_input.astype(jnp.float32), REC_VAL)
    g_heads = log_decay.transpose(1, 0, 2)
    zero_state = jnp.zeros((rec_heads, REC_KEY, REC_VAL), jnp.float32)
    local_out, local_state = recur_blocks(query_heads, k_heads, v_heads, g_heads, zero_state)
    reach_logarithm = jnp.cumsum(g_heads, axis=1)
    span_decay = jnp.exp(reach_logarithm[:, -1, :]) * carry_on
    prefix = prefix_2(
        (span_decay, local_state), "sp", chain, (jnp.ones_like(span_decay), zero_state)
    )
    incoming_state = prefix[1] * carry_on
    rec_raw = local_out + jnp.einsum(
        "ezp,ept->ezt",
        query_heads * jnp.exp(reach_logarithm),
        incoming_state,
        precision=TOP_PRECISION,
    )
    rec_mix = (
        rms_scale(rec_raw.transpose(1, 0, 2), rec_gain, RECUR_EPSILON)
        .astype(jnp.bfloat16)
        .reshape(tok_rows, rec_heads * REC_VAL)
    )
    mask_own = jnp.arange(tok_rows)[:, None] >= jnp.arange(tok_rows)[None, :]
    start_state = (
        jnp.full((att_heads, 2, tok_rows), -jnp.inf, jnp.float32),
        jnp.zeros((att_heads, 2, tok_rows), jnp.float32),
        jnp.zeros((att_heads, 2, tok_rows, ATT_VAL), jnp.float32),
    )
    online = absorb(
        start_state,
        att_query,
        att_key.reshape(tok_rows, att_heads, 2, PAIR),
        att_value.reshape(tok_rows, att_heads, ATT_VAL),
        mask_own,
    )
    everything = jnp.array(True)

    def take_block(state_now, keys_flat, values_flat, source):
        key_rows = keys_flat.reshape(tok_rows, att_heads, 2, PAIR)
        value_rows = values_flat.reshape(tok_rows, att_heads, ATT_VAL)
        return lax.cond(
            source >= first_dev,
            lambda held: absorb(held, att_query, key_rows, value_rows, everything),
            lambda held: held,
            state_now,
        )

    def relay_turn(hop_count, carried):
        moving_keys, moving_values, state_now = carried
        moving_keys, moving_values = from_behind((moving_keys, moving_values), "sp", 1)
        return (
            moving_keys,
            moving_values,
            take_block(state_now, moving_keys, moving_values, dev_index - hop_count - 1),
        )

    online = lax.fori_loop(0, seq_span - 1, relay_turn, (att_key, att_value, online))[2]
    best_score, sums_exp, weighted = online
    att_raw = (
        weighted[:, 0] / sums_exp[:, 0, :, None]
        - lambda_head[:, None, None] * weighted[:, 1] / sums_exp[:, 1, :, None]
    )
    att_mix = (
        rms_scale(att_raw.transpose(1, 0, 2), att_gain, ATTEND_EPSILON)
        .astype(jnp.bfloat16)
        .reshape(tok_rows, att_heads * ATT_VAL)
    )
    partial_value = jnp.dot(rec_mix, recurrence_output_weight, preferred_element_type=jnp.float32)
    partial_value = partial_value + jnp.dot(
        att_mix, out_att_weight, preferred_element_type=jnp.float32
    )
    return lax.psum(partial_value.astype(jnp.bfloat16), "tp")


MESH = pl.DeviceIdType.MESH
F32 = jnp.float32
BF16 = jnp.bfloat16
CUT = 128


def nt(a, b):
    return lax.dot_general(a, b, (((1,), (1,)), ((), ())), preferred_element_type=F32)


def tn(a, b):
    return lax.dot_general(a, b, (((0,), (0,)), ((), ())), preferred_element_type=F32)


def nn(a, b):
    return jnp.dot(a, b, preferred_element_type=F32)


def halves(x):
    high = x.astype(BF16)
    return high, (x - high.astype(F32)).astype(BF16)


def turn_map(values, cosine, sine_part):
    width = values.shape[-1]
    lane = lax.broadcasted_iota(jnp.int32, values.shape, 1)
    ahead = pltpu.roll(values, width - PAIR // 2, 1)
    back = pltpu.roll(values, PAIR // 2, 1)
    other = jnp.where(lane % PAIR < PAIR // 2, ahead, back)
    return values * cosine + other * sine_part


def fused_kernel(
    n, tps, span,
    tokens_far, wk, wv, wq, wf, wi, wr, rec_out, att_out, gain, gap, shift, rec_gain, att_gain, rates,
    lam, out,
    buf, xn, acc, wo, mix, kv, kv_prev, st, st_prev, total,
    tokens, near, cosine, sine_part,
    ssem, rsem, wo_s, wo_r, mix_s, mix_r, ex_s, ex_r, in_sem,
):
    weights = (wk, wv, wq, wf, wi, wr)
    chunks = len(weights)
    rows, width = tokens.shape
    depth, cols = wk.shape
    loads = [pltpu.make_async_copy(tokens_far, tokens, in_sem.at[0])]
    loads += [pltpu.make_async_copy(w, near.at[c], in_sem.at[1 + c]) for c, w in enumerate(weights)]
    me = lax.axis_index("sp")
    t = lax.axis_index("tp")
    up = (1 - me % 2)
    place = up * (me // 2) + (1 - up) * (n - 1 - me // 2)

    def at_place(p):
        q = (p + n) % n
        low = q // (n // 2)
        return (1 - low) * (2 * q) + low * (2 * (n - 1 - q) + 1)

    right, left = at_place(place + 1), at_place(place - 1)
    partner = t + 1 - 2 * (t % 2)
    across = (t + 2) % tps
    half = span // 2
    stage = (me + half) % span
    is_recv = jnp.logical_and(stage > 0, me >= half)
    is_send = jnp.logical_and(stage == 0, me + 1 < n)
    to_right, to_left = {"sp": right}, {"sp": left}
    to_partner, to_across = {"tp": partner}, {"tp": across}

    for load in loads:
        load.start()
    barrier = pltpu.get_barrier_semaphore()
    for target in (to_right, to_left, to_partner, to_across):
        pl.semaphore_signal(barrier, inc=1, device_id=target, device_id_type=MESH)

    @pl.when(is_send)
    def _():
        pl.semaphore_signal(barrier, inc=1, device_id={"sp": me + 1}, device_id_type=MESH)

    @pl.when(is_recv)
    def _():
        pl.semaphore_signal(barrier, inc=1, device_id={"sp": me - 1}, device_id_type=MESH)

    paired = jnp.logical_or(is_send, is_recv)

    @pl.when(paired)
    def _():
        pl.semaphore_wait(barrier, 5)

    @pl.when(jnp.logical_not(paired))
    def _():
        pl.semaphore_wait(barrier, 4)

    top = n // 2

    def slot(way, hop):
        return hop if way == 0 else n - hop

    def carried(way, hop):
        if hop < top:
            return tuple(range(chunks))
        if hop == top:
            return tuple(range(chunks // 2)) if way == 0 else tuple(range(chunks // 2, chunks))
        return ()

    def ring(way, hop, c):
        return pltpu.make_async_remote_copy(
            src_ref=weights[c] if hop == 1 else buf.at[slot(way, hop - 1), c],
            dst_ref=buf.at[slot(way, hop), c],
            send_sem=ssem.at[way, hop - 1, c],
            recv_sem=rsem.at[slot(way, hop), c],
            device_id=(to_right, to_left)[way],
            device_id_type=MESH,
        )

    def remote(src, dst, s, r, target):
        return pltpu.make_async_remote_copy(
            src_ref=src, dst_ref=dst, send_sem=s, recv_sem=r, device_id=target, device_id_type=MESH
        )

    outs_w = (rec_out, att_out)
    outs_near = [pltpu.make_async_copy(outs_w[k], wo.at[3, k], in_sem.at[7 + k]) for k in range(2)]

    def wo_copy(k, part):
        src = outs_w[part] if k < 2 else wo.at[1, part]
        return remote(src, wo.at[k, part], wo_s.at[k, part], wo_r.at[k, part], to_across if k == 1 else to_partner)

    def mix_copy(k, part):
        src = mix.at[3, part] if k < 2 else mix.at[1, part]
        return remote(src, mix.at[k, part], mix_s.at[k, part], mix_r.at[k, part], to_across if k == 1 else to_partner)

    for c in range(chunks):
        for way in range(2):
            ring(way, 1, c).start()
    for part in range(2):
        wo_copy(1, part).start()
        wo_copy(0, part).start()
        outs_near[part].start()

    loads[0].wait()
    values = tokens[...].astype(F32)
    mean_sq = jnp.mean(values * values, axis=-1, keepdims=True)
    normed = (values * lax.rsqrt(mean_sq + RECUR_EPSILON) * gain[...]).astype(BF16)
    for k in range(n):
        xn[k] = normed[:, k * depth : (k + 1) * depth]
    mine = xn[me]
    for c in range(chunks):
        loads[1 + c].wait()
        acc[c] = nn(mine, near[c])

    start = me - jnp.maximum(me - stage, 0)
    position = (lax.broadcasted_iota(jnp.int32, (rows, CUT), 0) + start * rows).astype(F32)
    angles = position * rates[...]
    signs = jnp.where(lax.broadcasted_iota(jnp.int32, (rows, CUT), 1) % PAIR < PAIR // 2, -1.0, 1.0)
    cosine[...] = jnp.cos(angles)
    sine_part[...] = jnp.sin(angles) * signs

    def project(way, hop, c):
        ring(way, hop, c).wait_recv()
        if c in carried(way, hop + 1):
            ring(way, hop + 1, c).start()
        origin = at_place(place - hop if way == 0 else place + hop)
        acc[c] = acc[c] + nn(xn[origin], buf[slot(way, hop), c])

    for hop in range(1, top):
        for c in range(chunks):
            for way in range(2):
                project(way, hop, c)
    for part in range(2):
        wo_copy(1, part).wait_recv()
        wo_copy(2, part).start()

    @pl.when(jnp.logical_not(is_recv))
    def _():
        kv_prev[...] = jnp.zeros(kv_prev.shape, BF16)
        st_prev[...] = jnp.zeros(st_prev.shape, F32)

    def ex_copy(k):
        src, dst = ((kv.at[0], kv_prev.at[0]), (kv.at[1], kv_prev.at[1]), (st, st_prev))[k]
        return remote(src, dst, ex_s.at[k], ex_r.at[k], {"sp": me + 1})

    heads = cols // CUT
    blocks = rows // CUT
    r_iota = lax.broadcasted_iota(jnp.int32, (CUT, CUT), 0)
    c_iota = lax.broadcasted_iota(jnp.int32, (CUT, CUT), 1)
    lower = r_iota >= c_iota
    ones = jnp.where(lower, 1.0, 0.0).astype(BF16)

    project(0, top, 0)
    for h in range(heads):
        lanes = slice(h * CUT, (h + 1) * CUT)
        kv[0, :, lanes] = turn_map(acc[0, :, lanes], cosine[...], sine_part[...]).astype(BF16)

    @pl.when(is_send)
    def _():
        ex_copy(0).start()

    project(1, top, 3)
    cums, keys = [], []
    for h in range(heads):
        lanes = slice(h * CUT, (h + 1) * CUT)
        forget = acc[3, :, lanes].astype(BF16).astype(F32)
        key = gap[:, lanes] * (1.0 / (1.0 + jnp.exp(forget)))
        high, low = halves(jnp.log(1.0 - key))
        for b in range(blocks):
            part = slice(b * CUT, (b + 1) * CUT)
            s_high, s_low = halves(jnp.broadcast_to(shift[h : h + 1, part], (CUT, CUT)))
            cums.append(nn(ones, high[part]) + nn(ones, low[part]) + nt(ones, s_high) + nt(ones, s_low))
            keys.append(key[part])

    project(0, top, 1)
    kv[1] = acc[1].astype(BF16)

    @pl.when(is_send)
    def _():
        ex_copy(1).start()

    project(1, top, 4)
    fresh, inputs = [], []
    for h in range(heads):
        lanes = slice(h * CUT, (h + 1) * CUT)
        own = jnp.zeros((CUT, CUT), F32)
        for b in range(blocks):
            i = h * blocks + b
            inp = acc[4, b * CUT : (b + 1) * CUT, lanes].astype(BF16)
            end = cums[i][CUT - 1 : CUT]
            to_end = (keys[i] * jnp.exp(end - cums[i])).astype(BF16)
            fresh.append(own)
            own = own * jnp.exp(end) + tn(inp, to_end)
            inputs.append(inp)
        st[h] = own

    @pl.when(is_send)
    def _():
        ex_copy(2).start()

    project(0, top, 2)
    project(1, top, 5)

    raws, pasts = [], []
    for h in range(heads):
        lanes = slice(h * CUT, (h + 1) * CUT)
        decay = jnp.zeros((1, CUT), F32)
        for b in range(blocks):
            i = h * blocks + b
            cum = cums[i]
            middle = cum[CUT // 2 - 1 : CUT // 2]
            q = acc[5, b * CUT : (b + 1) * CUT, lanes].astype(BF16).astype(F32)
            scores = nt((q * jnp.exp(cum - middle)).astype(BF16), (keys[i] * jnp.exp(middle - cum)).astype(BF16))
            scores = jnp.where(lower, scores, 0.0).astype(BF16)
            past = q * jnp.exp(cum)
            raw = nn(scores, inputs[i])
            if b:
                raw = raw + nt(past.astype(BF16), fresh[i].astype(BF16))
            raws.append(raw)
            pasts.append((past, decay))
            decay = decay + cum[CUT - 1 : CUT]

    for part in range(2):
        outs_near[part].wait()
        wo_copy(0, part).wait_recv()
        wo_copy(2, part).wait_recv()

    lane = lax.broadcasted_iota(jnp.int32, (rows, CUT), 1)
    own_mask = lax.broadcasted_iota(jnp.int32, (rows, rows), 0) >= lax.broadcasted_iota(jnp.int32, (rows, rows), 1)
    away = jnp.where(is_recv, 0.0, -1e30).astype(F32)

    own_scores = []
    turned = []
    for h in range(heads):
        lanes = slice(h * CUT, (h + 1) * CUT)
        query = turn_map(acc[2, :, lanes], cosine[...], sine_part[...]).astype(BF16)
        for c in range(2):
            picked = jnp.where((lane // PAIR) == c, query, jnp.zeros_like(query))
            turned.append(picked)

    @pl.when(is_recv)
    def _():
        for k in range(3):
            ex_copy(k).wait_recv()

    for h in range(heads):
        lanes = slice(h * CUT, (h + 1) * CUT)
        for b in range(blocks):
            i = h * blocks + b
            past, decay = pasts[i]
            came = (st_prev[h] * jnp.exp(decay)).astype(BF16)
            raw = raws[i] + nt(past.astype(BF16), came)
            mean_sq = jnp.mean(raw * raw, axis=-1, keepdims=True)
            mix[3, 0, b * CUT : (b + 1) * CUT, lanes] = (
                raw * lax.rsqrt(mean_sq + RECUR_EPSILON) * rec_gain[...]
            ).astype(BF16)
    mix_copy(1, 0).start()
    mix_copy(0, 0).start()

    for h in range(heads):
        lanes = slice(h * CUT, (h + 1) * CUT)
        found = []
        for c in range(2):
            picked = turned[h * 2 + c]
            s_own = jnp.where(own_mask, nt(picked, kv[0, :, lanes]) * PAIR ** (-0.5), -1e30)
            s_prev = nt(picked, kv_prev[0, :, lanes]) * PAIR ** (-0.5) + away
            best = jnp.maximum(jnp.max(s_own, axis=-1, keepdims=True), jnp.max(s_prev, axis=-1, keepdims=True))
            e_own, e_prev = jnp.exp(s_own - best), jnp.exp(s_prev - best)
            sums = jnp.sum(e_own, axis=-1, keepdims=True) + jnp.sum(e_prev, axis=-1, keepdims=True)
            weighted = nn(e_own.astype(BF16), kv[1, :, lanes]) + nn(e_prev.astype(BF16), kv_prev[1, :, lanes])
            found.append(weighted / sums)
        raw = found[0] - lam[h] * found[1]
        mean_sq = jnp.mean(raw * raw, axis=-1, keepdims=True)
        mix[3, 1, :, lanes] = (raw * lax.rsqrt(mean_sq + ATTEND_EPSILON) * att_gain[...]).astype(BF16)
    mix_copy(1, 1).start()
    mix_copy(0, 1).start()

    tile = 2 * cols
    tiles = width // tile

    def add(*terms, first=False, last=False):
        for j in range(tiles):
            span_cols = slice(j * tile, (j + 1) * tile)
            product = sum(nn(mix[k, part], wo[k, part, :, span_cols]) for k, part in terms)
            if not first:
                product = product + total[:, span_cols]
            if last:
                out[:, span_cols] = product.astype(BF16)
            else:
                total[:, span_cols] = product

    mix_copy(1, 0).wait_recv()
    mix_copy(2, 0).start()
    mix_copy(0, 0).wait_recv()
    add((3, 0), (3, 1), (0, 0), (1, 0), first=True)
    mix_copy(2, 0).wait_recv()
    mix_copy(0, 1).wait_recv()
    add((2, 0), (0, 1))
    mix_copy(1, 1).wait_recv()
    mix_copy(2, 1).start()
    add((1, 1))
    mix_copy(2, 1).wait_recv()
    add((2, 1), last=True)

    for hop in range(1, top + 1):
        for way in range(2):
            for c in carried(way, hop):
                ring(way, hop, c).wait_send()
    for k in range(3):
        for part in range(2):
            wo_copy(k, part).wait_send()
            mix_copy(k, part).wait_send()

    @pl.when(is_send)
    def _():
        for k in range(3):
            ex_copy(k).wait_send()


def per_device_fused(
    n, tps, span,
    tokens_in, norm_gain, rec_query_weight, rec_forget_weight, rec_input_weight,
    att_query_weight, att_key_weight, att_value_weight, recurrence_output_weight, out_att_weight,
    floor_gap, decay_shift, rec_gain, att_gain, lambda_head,
):
    rows, width = tokens_in.shape
    depth, cols = att_key_weight.shape
    half_width = PAIR // 2
    frequency = 1.0 / ROTARY_BASE ** (jnp.arange(half_width, dtype=F32) / half_width)
    rates = jnp.tile(frequency, CUT // half_width)[None]
    heads = cols // CUT
    vmem = pl.BlockSpec(memory_space=pltpu.VMEM)
    return pl.pallas_call(
        functools.partial(fused_kernel, n, tps, span),
        out_shape=jax.ShapeDtypeStruct((rows, width), BF16),
        in_specs=[pl.BlockSpec(memory_space=pltpu.HBM)] * 9 + [vmem] * 6 + [pl.BlockSpec(memory_space=pltpu.SMEM)],
        out_specs=vmem,
        scratch_shapes=[
            pltpu.VMEM((n, 6, depth, cols), BF16),
            pltpu.VMEM((n, rows, depth), BF16),
            pltpu.VMEM((6, rows, cols), F32),
            pltpu.VMEM((4, 2, cols, width), BF16),
            pltpu.VMEM((4, 2, rows, cols), BF16),
            pltpu.VMEM((2, rows, cols), BF16),
            pltpu.VMEM((2, rows, cols), BF16),
            pltpu.VMEM((heads, CUT, CUT), F32),
            pltpu.VMEM((heads, CUT, CUT), F32),
            pltpu.VMEM((rows, width), F32),
            pltpu.VMEM((rows, width), BF16),
            pltpu.VMEM((6, depth, cols), BF16),
            pltpu.VMEM((rows, CUT), F32),
            pltpu.VMEM((rows, CUT), F32),
            pltpu.SemaphoreType.DMA((2, n // 2, 6)),
            pltpu.SemaphoreType.DMA((n, 6)),
            pltpu.SemaphoreType.DMA((3, 2)),
            pltpu.SemaphoreType.DMA((3, 2)),
            pltpu.SemaphoreType.DMA((3, 2)),
            pltpu.SemaphoreType.DMA((3, 2)),
            pltpu.SemaphoreType.DMA((3,)),
            pltpu.SemaphoreType.DMA((3,)),
            pltpu.SemaphoreType.DMA((9,)),
        ],
        compiler_params=pltpu.CompilerParams(collective_id=0, has_side_effects=True, vmem_limit_bytes=60 << 20),
    )(
        tokens_in, att_key_weight, att_value_weight, att_query_weight,
        rec_forget_weight, rec_input_weight, rec_query_weight, recurrence_output_weight, out_att_weight,
        norm_gain[None], floor_gap[None], decay_shift, rec_gain[None], att_gain[None], rates, lambda_head,
    )


def solution(mesh):
    in_specs = (
        P("sp", None),
        P(),
        P("sp", "tp"),
        P("sp", "tp"),
        P("sp", "tp"),
        P("sp", "tp"),
        P("sp", "tp"),
        P("sp", "tp"),
        P("tp", None),
        P("tp", None),
        P("tp"),
        P("tp", "sp"),
        P(),
        P(),
        P("tp"),
    )
    out_specs = P("sp", None)
    n, tps = mesh.shape["sp"], mesh.shape["tp"]
    span = n // 4
    chosen = per_device
    if span == 2 and tps == 4:
        chosen = functools.partial(per_device_fused, n, tps, span)
    return jax.shard_map(
        chosen, mesh=mesh, in_specs=in_specs, out_specs=out_specs, check_vma=False
    )
```

```python
import functools

import jax
import jax.numpy as jnp
from jax import lax
from jax.experimental import pallas as pl
from jax.experimental.pallas import tpu as pltpu
from jax.sharding import PartitionSpec as P

REC_KEY = 128
REC_VAL = 128
PAIR = 64
ATT_VAL = 128
BLOCK = 64


RECUR_EPSILON = 1e-06
ATTEND_EPSILON = 1e-05
ROTARY_BASE = 10000.0
TOP_PRECISION = lax.Precision.HIGHEST


def prefix_2(array, axis, combine, identity):
    count, position = (lax.axis_size(axis), lax.axis_index(axis))
    everything = jax.tree.map(
        lambda part, kind: lax.all_gather(part.astype(kind), axis),
        array,
        (jnp.bfloat16, jnp.bfloat16),
    )
    start = jax.tree.map(
        lambda part, zero: jnp.broadcast_to(jnp.asarray(zero, part.dtype), part.shape),
        array,
        identity,
    )

    def turn(k, before):
        reached = k < position
        new = combine(
            before, jax.tree.map(lambda part, own: part[k].astype(own.dtype), everything, array)
        )
        return jax.tree.map(lambda a, b: jnp.where(reached, a, b), new, before)

    return lax.fori_loop(0, count, turn, start)


def from_behind(block, axis, distance):
    devices = range(lax.axis_size(axis))
    route = [(i - distance, i) for i in devices if i - distance in devices]
    return lax.ppermute(block, axis, route)


def rms_scale(values, scales, epsilon):
    mean_sq = jnp.mean(values * values, axis=-1, keepdims=True)
    return values * lax.rsqrt(mean_sq + epsilon) * scales


def rotary(values, positions):
    half_width = values.shape[-1] // 2
    frequency = 1.0 / ROTARY_BASE ** (jnp.arange(half_width, dtype=jnp.float32) / half_width)
    angles = positions[:, None] * frequency[None, :]
    cosine = jnp.cos(angles)[:, None, :]
    sine_part = jnp.sin(angles)[:, None, :]
    first_half = values[..., :half_width]
    second_half = values[..., half_width:]
    return jnp.concatenate(
        [
            first_half * cosine - second_half * sine_part,
            second_half * cosine + first_half * sine_part,
        ],
        axis=-1,
    )


def recur_blocks(queries, gate_key_rows, inputs, log_decay, carry_in):
    head_count = queries.shape[0]
    length = queries.shape[1]
    block_count = length // BLOCK

    def split_blocks(array):
        return array.reshape(head_count, block_count, BLOCK, array.shape[-1]).transpose(1, 0, 2, 3)

    causal = jnp.tril(jnp.ones((BLOCK, BLOCK), dtype=bool))

    def advance(carried, bundle):
        q_block, k_block, v_block, g_block = bundle
        cum_log = jnp.cumsum(g_block, axis=1)
        q_decayed = q_block * jnp.exp(cum_log)
        k_growth = k_block * jnp.exp(-cum_log)
        from_past = jnp.einsum("hcd,hde->hce", q_decayed, carried, precision=TOP_PRECISION)
        scores = jnp.einsum("htd,hsd->hts", q_decayed, k_growth, precision=TOP_PRECISION)
        scores = jnp.where(causal[None], scores, 0.0)
        within = jnp.einsum("hts,hse->hte", scores, v_block, precision=TOP_PRECISION)
        end_log = cum_log[:, -1:, :]
        k_to_end = k_block * jnp.exp(end_log - cum_log)
        fresh = jnp.exp(end_log[:, 0, :])[:, :, None] * carried + jnp.einsum(
            "hsd,hse->hde", k_to_end, v_block, precision=TOP_PRECISION
        )
        return (fresh, from_past + within)

    final_state, outputs = lax.scan(
        advance,
        carry_in,
        (
            split_blocks(queries),
            split_blocks(gate_key_rows),
            split_blocks(inputs),
            split_blocks(log_decay),
        ),
    )
    return (
        outputs.transpose(1, 0, 2, 3).reshape(head_count, length, inputs.shape[-1]),
        final_state,
    )


def chain(earlier, latter):
    return (earlier[0] * latter[0], latter[0][:, :, None] * earlier[1] + latter[1])


def absorb(running_total, queries, key_rows, value_rows, allowed):
    best_score, sums_exp, weighted = running_total
    scores = jnp.einsum(
        "qhcd,khcd->hcqk", queries, key_rows, preferred_element_type=jnp.float32
    ) * queries.shape[-1] ** (-0.5)
    scores = jnp.where(allowed, scores, -jnp.inf)
    new_best = jnp.maximum(best_score, jnp.max(scores, axis=-1))
    rescale = jnp.exp(best_score - new_best)
    expo_vals = jnp.exp(scores - new_best[..., None])
    sums_exp = sums_exp * rescale + jnp.sum(expo_vals, axis=-1)
    weighted = weighted * rescale[..., None] + jnp.einsum(
        "hcqk,khe->hcqe",
        expo_vals.astype(jnp.bfloat16),
        value_rows,
        preferred_element_type=jnp.float32,
    )
    return (new_best, sums_exp, weighted)


def per_device(
    tokens_in,
    norm_gain,
    rec_query_weight,
    rec_forget_weight,
    rec_input_weight,
    att_query_weight,
    att_key_weight,
    att_value_weight,
    recurrence_output_weight,
    out_att_weight,
    floor_gap,
    decay_shift,
    rec_gain,
    att_gain,
    lambda_head,
):
    tok_rows = tokens_in.shape[0]
    seq_span = lax.axis_size("sp") // 4
    half_span = seq_span // 2
    dev_index = lax.axis_index("sp")
    first_dev = jnp.maximum(0, (dev_index + half_span) // seq_span * seq_span - half_span)
    carry_on = jnp.where(dev_index == first_dev, 0.0, 1.0).astype(jnp.float32)
    gathered = (
        lax.all_gather(rec_query_weight, "sp", axis=0, tiled=True),
        lax.all_gather(rec_forget_weight, "sp", axis=0, tiled=True),
        lax.all_gather(rec_input_weight, "sp", axis=0, tiled=True),
        lax.all_gather(att_query_weight, "sp", axis=0, tiled=True),
        lax.all_gather(att_key_weight, "sp", axis=0, tiled=True),
        lax.all_gather(att_value_weight, "sp", axis=0, tiled=True),
    )
    w_query, w_forget, w_input, w_att_query, w_att_key, w_att_value = gathered
    normed = rms_scale(tokens_in.astype(jnp.float32), norm_gain, RECUR_EPSILON).astype(jnp.bfloat16)

    def project(weight):
        return jnp.dot(normed, weight, preferred_element_type=jnp.float32)

    rec_query = project(w_query).astype(jnp.bfloat16)
    rec_forget = project(w_forget).astype(jnp.bfloat16)
    rec_input = project(w_input).astype(jnp.bfloat16)
    att_heads = w_att_query.shape[1] // (2 * PAIR)
    positions = ((dev_index - first_dev) * tok_rows + jnp.arange(tok_rows, dtype=jnp.int32)).astype(
        jnp.float32
    )
    att_query = (
        rotary(project(w_att_query).reshape(tok_rows, att_heads * 2, PAIR), positions)
        .astype(jnp.bfloat16)
        .reshape(tok_rows, att_heads, 2, PAIR)
    )
    att_key = (
        rotary(project(w_att_key).reshape(tok_rows, att_heads * 2, PAIR), positions)
        .astype(jnp.bfloat16)
        .reshape(tok_rows, att_heads * 2 * PAIR)
    )
    att_value = project(w_att_value).astype(jnp.bfloat16)
    rec_heads = w_query.shape[1] // REC_KEY
    gate_key = floor_gap[None, :] * jax.nn.sigmoid(-rec_forget.astype(jnp.float32))
    log_decay = (
        jnp.log1p(-gate_key).reshape(tok_rows, rec_heads, REC_KEY) + decay_shift.T[:, :, None]
    )

    def by_head(array, column_count):
        return array.reshape(tok_rows, rec_heads, column_count).transpose(1, 0, 2)

    query_heads = by_head(rec_query.astype(jnp.float32), REC_KEY)
    k_heads = by_head(gate_key, REC_KEY)
    v_heads = by_head(rec_input.astype(jnp.float32), REC_VAL)
    g_heads = log_decay.transpose(1, 0, 2)
    zero_state = jnp.zeros((rec_heads, REC_KEY, REC_VAL), jnp.float32)
    local_out, local_state = recur_blocks(query_heads, k_heads, v_heads, g_heads, zero_state)
    reach_logarithm = jnp.cumsum(g_heads, axis=1)
    span_decay = jnp.exp(reach_logarithm[:, -1, :]) * carry_on
    prefix = prefix_2(
        (span_decay, local_state), "sp", chain, (jnp.ones_like(span_decay), zero_state)
    )
    incoming_state = prefix[1] * carry_on
    rec_raw = local_out + jnp.einsum(
        "ezp,ept->ezt",
        query_heads * jnp.exp(reach_logarithm),
        incoming_state,
        precision=TOP_PRECISION,
    )
    rec_mix = (
        rms_scale(rec_raw.transpose(1, 0, 2), rec_gain, RECUR_EPSILON)
        .astype(jnp.bfloat16)
        .reshape(tok_rows, rec_heads * REC_VAL)
    )
    mask_own = jnp.arange(tok_rows)[:, None] >= jnp.arange(tok_rows)[None, :]
    start_state = (
        jnp.full((att_heads, 2, tok_rows), -jnp.inf, jnp.float32),
        jnp.zeros((att_heads, 2, tok_rows), jnp.float32),
        jnp.zeros((att_heads, 2, tok_rows, ATT_VAL), jnp.float32),
    )
    online = absorb(
        start_state,
        att_query,
        att_key.reshape(tok_rows, att_heads, 2, PAIR),
        att_value.reshape(tok_rows, att_heads, ATT_VAL),
        mask_own,
    )
    everything = jnp.array(True)

    def take_block(state_now, keys_flat, values_flat, source):
        key_rows = keys_flat.reshape(tok_rows, att_heads, 2, PAIR)
        value_rows = values_flat.reshape(tok_rows, att_heads, ATT_VAL)
        return lax.cond(
            source >= first_dev,
            lambda held: absorb(held, att_query, key_rows, value_rows, everything),
            lambda held: held,
            state_now,
        )

    def relay_turn(hop_count, carried):
        moving_keys, moving_values, state_now = carried
        moving_keys, moving_values = from_behind((moving_keys, moving_values), "sp", 1)
        return (
            moving_keys,
            moving_values,
            take_block(state_now, moving_keys, moving_values, dev_index - hop_count - 1),
        )

    online = lax.fori_loop(0, seq_span - 1, relay_turn, (att_key, att_value, online))[2]
    best_score, sums_exp, weighted = online
    att_raw = (
        weighted[:, 0] / sums_exp[:, 0, :, None]
        - lambda_head[:, None, None] * weighted[:, 1] / sums_exp[:, 1, :, None]
    )
    att_mix = (
        rms_scale(att_raw.transpose(1, 0, 2), att_gain, ATTEND_EPSILON)
        .astype(jnp.bfloat16)
        .reshape(tok_rows, att_heads * ATT_VAL)
    )
    partial_value = jnp.dot(rec_mix, recurrence_output_weight, preferred_element_type=jnp.float32)
    partial_value = partial_value + jnp.dot(
        att_mix, out_att_weight, preferred_element_type=jnp.float32
    )
    return lax.psum(partial_value.astype(jnp.bfloat16), "tp")


MESH = pl.DeviceIdType.MESH
F32 = jnp.float32
BF16 = jnp.bfloat16
CUT = 128


def nt(a, b):
    return lax.dot_general(a, b, (((1,), (1,)), ((), ())), preferred_element_type=F32)


def tn(a, b):
    return lax.dot_general(a, b, (((0,), (0,)), ((), ())), preferred_element_type=F32)


def nn(a, b):
    return jnp.dot(a, b, preferred_element_type=F32)


def halves(x):
    high = x.astype(BF16)
    return high, (x - high.astype(F32)).astype(BF16)


def turn_map(values, cosine, sine_part):
    width = values.shape[-1]
    lane = lax.broadcasted_iota(jnp.int32, values.shape, 1)
    ahead = pltpu.roll(values, width - PAIR // 2, 1)
    back = pltpu.roll(values, PAIR // 2, 1)
    other = jnp.where(lane % PAIR < PAIR // 2, ahead, back)
    return values * cosine + other * sine_part


def fused_kernel(
    n, tps, span,
    tokens_far, wk, wv, wq, wf, wi, wr, rec_out, att_out, gain, gap, shift, rec_gain, att_gain, rates,
    lam, out,
    buf, xn, acc, wo, mix, kv, kv_prev, st, st_prev, total,
    tokens, near, cosine, sine_part,
    ssem, rsem, wo_s, wo_r, mix_s, mix_r, ex_s, ex_r, in_sem,
):
    weights = (wk, wf, wq, wv, wi, wr)
    chunks = len(weights)
    rows, width = tokens.shape
    depth, cols = wk.shape
    loads = [pltpu.make_async_copy(tokens_far, tokens, in_sem.at[0])]
    loads += [pltpu.make_async_copy(w, near.at[c], in_sem.at[1 + c]) for c, w in enumerate(weights)]
    me = lax.axis_index("sp")
    t = lax.axis_index("tp")
    up = (1 - me % 2)
    place = up * (me // 2) + (1 - up) * (n - 1 - me // 2)

    def at_place(p):
        q = (p + n) % n
        low = q // (n // 2)
        return (1 - low) * (2 * q) + low * (2 * (n - 1 - q) + 1)

    right, left = at_place(place + 1), at_place(place - 1)
    partner = t + 1 - 2 * (t % 2)
    across = (t + 2) % tps
    half = span // 2
    stage = (me + half) % span
    is_recv = jnp.logical_and(stage > 0, me >= half)
    is_send = jnp.logical_and(stage == 0, me + 1 < n)
    to_right, to_left = {"sp": right}, {"sp": left}
    to_partner, to_across = {"tp": partner}, {"tp": across}

    for load in loads:
        load.start()
    barrier = pltpu.get_barrier_semaphore()
    for target in (to_right, to_left, to_partner, to_across):
        pl.semaphore_signal(barrier, inc=1, device_id=target, device_id_type=MESH)

    @pl.when(is_send)
    def _():
        pl.semaphore_signal(barrier, inc=1, device_id={"sp": me + 1}, device_id_type=MESH)

    @pl.when(is_recv)
    def _():
        pl.semaphore_signal(barrier, inc=1, device_id={"sp": me - 1}, device_id_type=MESH)

    paired = jnp.logical_or(is_send, is_recv)

    @pl.when(paired)
    def _():
        pl.semaphore_wait(barrier, 5)

    @pl.when(jnp.logical_not(paired))
    def _():
        pl.semaphore_wait(barrier, 4)

    top = n // 2

    def slot(way, hop):
        return hop if way == 0 else n - hop

    def carried(way, hop):
        if hop < top:
            return tuple(range(chunks))
        if hop == top:
            return tuple(range(chunks // 2)) if way == 0 else tuple(range(chunks // 2, chunks))
        return ()

    def ring(way, hop, c):
        return pltpu.make_async_remote_copy(
            src_ref=weights[c] if hop == 1 else buf.at[slot(way, hop - 1), c],
            dst_ref=buf.at[slot(way, hop), c],
            send_sem=ssem.at[way, hop - 1, c],
            recv_sem=rsem.at[slot(way, hop), c],
            device_id=(to_right, to_left)[way],
            device_id_type=MESH,
        )

    def remote(src, dst, s, r, target):
        return pltpu.make_async_remote_copy(
            src_ref=src, dst_ref=dst, send_sem=s, recv_sem=r, device_id=target, device_id_type=MESH
        )

    outs_w = (rec_out, att_out)
    outs_near = [pltpu.make_async_copy(outs_w[k], wo.at[3, k], in_sem.at[7 + k]) for k in range(2)]

    def wo_copy(k, part):
        src = outs_w[part] if k < 2 else wo.at[1, part]
        return remote(src, wo.at[k, part], wo_s.at[k, part], wo_r.at[k, part], to_across if k == 1 else to_partner)

    def mix_copy(k, part):
        src = mix.at[3, part] if k < 2 else mix.at[1, part]
        return remote(src, mix.at[k, part], mix_s.at[k, part], mix_r.at[k, part], to_across if k == 1 else to_partner)

    for c in range(chunks):
        for way in range(2):
            ring(way, 1, c).start()
    for part in range(2):
        wo_copy(1, part).start()
        wo_copy(0, part).start()
        outs_near[part].start()

    loads[0].wait()
    values = tokens[...].astype(F32)
    mean_sq = jnp.mean(values * values, axis=-1, keepdims=True)
    normed = (values * lax.rsqrt(mean_sq + RECUR_EPSILON) * gain[...]).astype(BF16)
    for k in range(n):
        xn[k] = normed[:, k * depth : (k + 1) * depth]
    mine = xn[me]
    for c in range(chunks):
        loads[1 + c].wait()
        acc[c] = nn(mine, near[c])

    start = me - jnp.maximum(me - stage, 0)
    position = (lax.broadcasted_iota(jnp.int32, (rows, CUT), 0) + start * rows).astype(F32)
    angles = position * rates[...]
    signs = jnp.where(lax.broadcasted_iota(jnp.int32, (rows, CUT), 1) % PAIR < PAIR // 2, -1.0, 1.0)
    cosine[...] = jnp.cos(angles)
    sine_part[...] = jnp.sin(angles) * signs

    def project(way, hop, c):
        ring(way, hop, c).wait_recv()
        if c in carried(way, hop + 1):
            ring(way, hop + 1, c).start()
        origin = at_place(place - hop if way == 0 else place + hop)
        acc[c] = acc[c] + nn(xn[origin], buf[slot(way, hop), c])

    for hop in range(1, top):
        for c in range(chunks):
            for way in range(2):
                project(way, hop, c)
    for part in range(2):
        wo_copy(1, part).wait_recv()
        wo_copy(2, part).start()

    @pl.when(jnp.logical_not(is_recv))
    def _():
        kv_prev[...] = jnp.zeros(kv_prev.shape, BF16)
        st_prev[...] = jnp.zeros(st_prev.shape, BF16)

    def ex_copy(k):
        src, dst = ((kv.at[0], kv_prev.at[0]), (kv.at[1], kv_prev.at[1]), (st, st_prev))[k]
        return remote(src, dst, ex_s.at[k], ex_r.at[k], {"sp": me + 1})

    heads = cols // CUT
    blocks = rows // CUT
    r_iota = lax.broadcasted_iota(jnp.int32, (CUT, CUT), 0)
    c_iota = lax.broadcasted_iota(jnp.int32, (CUT, CUT), 1)
    lower = r_iota >= c_iota
    ones = jnp.where(lower, 1.0, 0.0).astype(BF16)

    project(0, top, 0)
    for h in range(heads):
        lanes = slice(h * CUT, (h + 1) * CUT)
        kv[0, :, lanes] = turn_map(acc[0, :, lanes], cosine[...], sine_part[...]).astype(BF16)

    @pl.when(is_send)
    def _():
        ex_copy(0).start()

    project(1, top, 3)
    kv[1] = acc[3].astype(BF16)

    @pl.when(is_send)
    def _():
        ex_copy(1).start()

    project(0, top, 1)
    cums, keys = [], []
    for h in range(heads):
        lanes = slice(h * CUT, (h + 1) * CUT)
        forget = acc[1, :, lanes].astype(BF16).astype(F32)
        key = gap[:, lanes] * (1.0 / (1.0 + jnp.exp(forget)))
        high, low = halves(jnp.log(1.0 - key))
        for b in range(blocks):
            part = slice(b * CUT, (b + 1) * CUT)
            s_high, s_low = halves(jnp.broadcast_to(shift[h : h + 1, part], (CUT, CUT)))
            cums.append(nn(ones, high[part]) + nn(ones, low[part]) + nt(ones, s_high) + nt(ones, s_low))
            keys.append(key[part])

    project(1, top, 4)
    fresh, inputs = [], []
    for h in range(heads):
        lanes = slice(h * CUT, (h + 1) * CUT)
        own = jnp.zeros((CUT, CUT), F32)
        for b in range(blocks):
            i = h * blocks + b
            inp = acc[4, b * CUT : (b + 1) * CUT, lanes].astype(BF16)
            end = cums[i][CUT - 1 : CUT]
            to_end = (keys[i] * jnp.exp(end - cums[i])).astype(BF16)
            fresh.append(own)
            own = own * jnp.exp(end) + tn(inp, to_end)
            inputs.append(inp)
        st[h] = own.astype(BF16)

    @pl.when(is_send)
    def _():
        ex_copy(2).start()

    project(0, top, 2)
    project(1, top, 5)

    raws, pasts = [], []
    for h in range(heads):
        lanes = slice(h * CUT, (h + 1) * CUT)
        decay = jnp.zeros((1, CUT), F32)
        for b in range(blocks):
            i = h * blocks + b
            cum = cums[i]
            middle = cum[CUT // 2 - 1 : CUT // 2]
            q = acc[5, b * CUT : (b + 1) * CUT, lanes].astype(BF16).astype(F32)
            scores = nt((q * jnp.exp(cum - middle)).astype(BF16), (keys[i] * jnp.exp(middle - cum)).astype(BF16))
            scores = jnp.where(lower, scores, 0.0).astype(BF16)
            past = q * jnp.exp(cum)
            raw = nn(scores, inputs[i])
            if b:
                raw = raw + nt(past.astype(BF16), fresh[i].astype(BF16))
            raws.append(raw)
            pasts.append((past, decay))
            decay = decay + cum[CUT - 1 : CUT]

    for part in range(2):
        outs_near[part].wait()
        wo_copy(0, part).wait_recv()
        wo_copy(2, part).wait_recv()

    lane = lax.broadcasted_iota(jnp.int32, (rows, CUT), 1)
    own_mask = lax.broadcasted_iota(jnp.int32, (rows, rows), 0) >= lax.broadcasted_iota(jnp.int32, (rows, rows), 1)
    away = jnp.where(is_recv, 0.0, -1e30).astype(F32)

    own_scores = []
    turned = []
    for h in range(heads):
        lanes = slice(h * CUT, (h + 1) * CUT)
        query = turn_map(acc[2, :, lanes], cosine[...], sine_part[...]).astype(BF16)
        for c in range(2):
            picked = jnp.where((lane // PAIR) == c, query, jnp.zeros_like(query))
            turned.append(picked)

    @pl.when(is_recv)
    def _():
        for k in range(3):
            ex_copy(k).wait_recv()

    for h in range(heads):
        lanes = slice(h * CUT, (h + 1) * CUT)
        for b in range(blocks):
            i = h * blocks + b
            past, decay = pasts[i]
            came = (st_prev[h].astype(F32) * jnp.exp(decay)).astype(BF16)
            raw = raws[i] + nt(past.astype(BF16), came)
            mean_sq = jnp.mean(raw * raw, axis=-1, keepdims=True)
            mix[3, 0, b * CUT : (b + 1) * CUT, lanes] = (
                raw * lax.rsqrt(mean_sq + RECUR_EPSILON) * rec_gain[...]
            ).astype(BF16)
    mix_copy(1, 0).start()
    mix_copy(0, 0).start()

    for h in range(heads):
        lanes = slice(h * CUT, (h + 1) * CUT)
        found = []
        for c in range(2):
            picked = turned[h * 2 + c]
            s_own = jnp.where(own_mask, nt(picked, kv[0, :, lanes]) * PAIR ** (-0.5), -1e30)
            s_prev = nt(picked, kv_prev[0, :, lanes]) * PAIR ** (-0.5) + away
            best = jnp.maximum(jnp.max(s_own, axis=-1, keepdims=True), jnp.max(s_prev, axis=-1, keepdims=True))
            e_own, e_prev = jnp.exp(s_own - best), jnp.exp(s_prev - best)
            sums = jnp.sum(e_own, axis=-1, keepdims=True) + jnp.sum(e_prev, axis=-1, keepdims=True)
            weighted = nn(e_own.astype(BF16), kv[1, :, lanes]) + nn(e_prev.astype(BF16), kv_prev[1, :, lanes])
            found.append(weighted / sums)
        raw = found[0] - lam[h] * found[1]
        mean_sq = jnp.mean(raw * raw, axis=-1, keepdims=True)
        mix[3, 1, :, lanes] = (raw * lax.rsqrt(mean_sq + ATTEND_EPSILON) * att_gain[...]).astype(BF16)
    mix_copy(1, 1).start()
    mix_copy(0, 1).start()

    tile = 2 * cols
    tiles = width // tile

    def add(*terms, first=False, last=False):
        for j in range(tiles):
            span_cols = slice(j * tile, (j + 1) * tile)
            product = sum(nn(mix[k, part], wo[k, part, :, span_cols]) for k, part in terms)
            if not first:
                product = product + total[:, span_cols]
            if last:
                out[:, span_cols] = product.astype(BF16)
            else:
                total[:, span_cols] = product

    mix_copy(1, 0).wait_recv()
    mix_copy(2, 0).start()
    mix_copy(0, 0).wait_recv()
    add((3, 0), (3, 1), (0, 0), (1, 0), first=True)
    mix_copy(2, 0).wait_recv()
    mix_copy(0, 1).wait_recv()
    add((2, 0), (0, 1))
    mix_copy(1, 1).wait_recv()
    mix_copy(2, 1).start()
    add((1, 1))
    mix_copy(2, 1).wait_recv()
    add((2, 1), last=True)

    for hop in range(1, top + 1):
        for way in range(2):
            for c in carried(way, hop):
                ring(way, hop, c).wait_send()
    for k in range(3):
        for part in range(2):
            wo_copy(k, part).wait_send()
            mix_copy(k, part).wait_send()

    @pl.when(is_send)
    def _():
        for k in range(3):
            ex_copy(k).wait_send()


def per_device_fused(
    n, tps, span,
    tokens_in, norm_gain, rec_query_weight, rec_forget_weight, rec_input_weight,
    att_query_weight, att_key_weight, att_value_weight, recurrence_output_weight, out_att_weight,
    floor_gap, decay_shift, rec_gain, att_gain, lambda_head,
):
    rows, width = tokens_in.shape
    depth, cols = att_key_weight.shape
    half_width = PAIR // 2
    frequency = 1.0 / ROTARY_BASE ** (jnp.arange(half_width, dtype=F32) / half_width)
    rates = jnp.tile(frequency, CUT // half_width)[None]
    heads = cols // CUT
    vmem = pl.BlockSpec(memory_space=pltpu.VMEM)
    return pl.pallas_call(
        functools.partial(fused_kernel, n, tps, span),
        out_shape=jax.ShapeDtypeStruct((rows, width), BF16),
        in_specs=[pl.BlockSpec(memory_space=pltpu.HBM)] * 9 + [vmem] * 6 + [pl.BlockSpec(memory_space=pltpu.SMEM)],
        out_specs=vmem,
        scratch_shapes=[
            pltpu.VMEM((n, 6, depth, cols), BF16),
            pltpu.VMEM((n, rows, depth), BF16),
            pltpu.VMEM((6, rows, cols), F32),
            pltpu.VMEM((4, 2, cols, width), BF16),
            pltpu.VMEM((4, 2, rows, cols), BF16),
            pltpu.VMEM((2, rows, cols), BF16),
            pltpu.VMEM((2, rows, cols), BF16),
            pltpu.VMEM((heads, CUT, CUT), BF16),
            pltpu.VMEM((heads, CUT, CUT), BF16),
            pltpu.VMEM((rows, width), F32),
            pltpu.VMEM((rows, width), BF16),
            pltpu.VMEM((6, depth, cols), BF16),
            pltpu.VMEM((rows, CUT), F32),
            pltpu.VMEM((rows, CUT), F32),
            pltpu.SemaphoreType.DMA((2, n // 2, 6)),
            pltpu.SemaphoreType.DMA((n, 6)),
            pltpu.SemaphoreType.DMA((3, 2)),
            pltpu.SemaphoreType.DMA((3, 2)),
            pltpu.SemaphoreType.DMA((3, 2)),
            pltpu.SemaphoreType.DMA((3, 2)),
            pltpu.SemaphoreType.DMA((3,)),
            pltpu.SemaphoreType.DMA((3,)),
            pltpu.SemaphoreType.DMA((9,)),
        ],
        compiler_params=pltpu.CompilerParams(collective_id=0, has_side_effects=True, vmem_limit_bytes=60 << 20),
    )(
        tokens_in, att_key_weight, att_value_weight, att_query_weight,
        rec_forget_weight, rec_input_weight, rec_query_weight, recurrence_output_weight, out_att_weight,
        norm_gain[None], floor_gap[None], decay_shift, rec_gain[None], att_gain[None], rates, lambda_head,
    )


def solution(mesh):
    in_specs = (
        P("sp", None),
        P(),
        P("sp", "tp"),
        P("sp", "tp"),
        P("sp", "tp"),
        P("sp", "tp"),
        P("sp", "tp"),
        P("sp", "tp"),
        P("tp", None),
        P("tp", None),
        P("tp"),
        P("tp", "sp"),
        P(),
        P(),
        P("tp"),
    )
    out_specs = P("sp", None)
    n, tps = mesh.shape["sp"], mesh.shape["tp"]
    span = n // 4
    chosen = per_device
    if span == 2 and tps == 4:
        chosen = functools.partial(per_device_fused, n, tps, span)
    return jax.shard_map(
        chosen, mesh=mesh, in_specs=in_specs, out_specs=out_specs, check_vma=False
    )
```
